512 devices in a mesh: ep: 32 (over z, x), tp: 16 (over y, core).
Axes of the slice: x: 4, y: 8, z: 8, core: 2. Of those that a mesh axis runs over, the one named last changes fastest.
Arguments:
- tokens: bfloat16 [8192, 2048], P('ep')
- norm_gain: float32 [2048], replicated, may hold values from 0.1 to 1.9
- chosen: int32 [32, 1024], replicated, may hold values from 0 to 8191, as said below
- route_weight: float32 [32, 1024], P('ep'), may hold values from 0.2 to 1
- gate_weight: bfloat16 [32, 2048, 4096], P('ep', None, 'tp'), may hold values from -0.125 to 0.125
- up_weight: bfloat16 [32, 2048, 4096], P('ep', None, 'tp'), may hold values from -0.125 to 0.125
- down_weight: bfloat16 [32, 4096, 2048], P('ep', 'tp'), may hold values from -0.09375 to 0.09375
Outputs:
- combined: bfloat16 [8192, 2048], P('ep', 'tp')
The draws below stay inside these ranges and needn't reach their ends.
Inputs may be any that keep to these rules, and one draw needn't show every extreme that they name: Each row of chosen lists 1024 distinct token numbers in ascending order. Of the 256 consecutive tokens of one index of ep, a row holds at most 48, and every draw has rows that hold exactly 48 of them.
All inputs are finite; a program needn't handle non-finite values.
Results may differ from the reference program's by a relative error of at most 0.02.
Values may be sent and summed in bfloat16 or wider, within the bound.
A program may use at most 64 MiB of HBM per device.

```python
import math
import jax
import jax.numpy as jnp
from jax import lax

D = 2048
FF = 4096
TOK_DEV = 256
EXPERTS = 32
TOKENS = 8192
CAP = 1024
FF_BLK = 256
N_TP = 16


def draw_tokens(key, part):
    keys = jax.random.split(jax.random.fold_in(key, 11), 3)
    row_scale = jnp.exp(jax.random.uniform(keys[0], (TOKENS, 1), jnp.float32, 0.0, math.log(10.0)))
    col_scale = jnp.exp(jax.random.uniform(keys[1], (1, D), jnp.float32, 0.0, math.log(10.0)))
    values = jax.random.normal(keys[2], (TOKENS, D), jnp.float32)
    return (values * row_scale * col_scale / 3.0).astype(jnp.bfloat16)


def draw_chosen(key, part):
    share = TOK_DEV // 8
    pairs = EXPERTS // 2
    steps = jnp.arange(pairs, dtype=jnp.int32)
    spread = share // 2 * steps // max(pairs - 1, 1)
    base = jnp.stack([share + spread, share - spread], axis=1).reshape(EXPERTS)
    expert_keys = jax.random.split(jax.random.fold_in(key, 23), EXPERTS)

    def one_expert(expert_key):
        order_key, rank_key = jax.random.split(expert_key)
        counts = base[jax.random.permutation(order_key, EXPERTS)]
        block_keys = jax.random.split(rank_key, EXPERTS)
        ranks = jax.vmap(lambda block_key: jax.random.permutation(block_key, TOK_DEV))(block_keys)
        picked = (ranks < counts[:, None]).reshape(TOKENS).astype(jnp.int32)
        order = jnp.argsort(1 - picked, stable=True)
        return order[:CAP].astype(jnp.int32)
    return jax.vmap(one_expert)(expert_keys)


def steps_of(stream_key, extent, cuts, least, top_value):
    def one(dim, blocks):
        heights = jax.random.uniform(jax.random.fold_in(jax.random.fold_in(stream_key, 6), dim), (blocks,), jnp.float32, least / len(cuts), top_value / len(cuts))
        return jnp.repeat(jnp.exp(heights), extent[dim] // blocks).reshape((-1,) + (1,) * (len(extent) - dim - 1))

    gain = one(*cuts[0])
    for cut in cuts[1:]:
        gain = gain * one(*cut)
    return gain


def scatter_about(stream_key, shape, width, reach, pieces=(), kind=jnp.bfloat16):
    array = width * jax.random.normal(stream_key, shape, jnp.float32)
    if pieces:
        array = array * steps_of(stream_key, shape, pieces, -0.22, 0.18)
    return jnp.clip(array, -reach, reach).astype(kind)


def setup_inputs(seed: int = 0) -> dict:
    key_list = jax.random.split(jax.random.key(seed), 8)
    return {
        "tokens": draw_tokens(jax.random.fold_in(key_list[7], 71), 0),
        "norm_gain": jnp.clip(1.0 + 0.18 * jax.random.normal(key_list[1], (D,), jnp.float32), 0.1, 1.9),
        "chosen": draw_chosen(jax.random.fold_in(key_list[7], 71), 0),
        "route_weight": jnp.clip(0.2 + 0.8 * jax.random.uniform(key_list[3], (EXPERTS, CAP), jnp.float32) ** steps_of(key_list[3], (EXPERTS, CAP), ((0, 32),), -0.2, 0.2), 0.2, 1.0),
        "gate_weight": scatter_about(key_list[4], (EXPERTS, D, FF), D ** -0.5, 0.125, ((0, 32), (2, 16))),
        "up_weight": scatter_about(key_list[5], (EXPERTS, D, FF), D ** -0.5, 0.125, ((0, 32), (2, 16))),
        "down_weight": scatter_about(key_list[6], (EXPERTS, FF, D), FF ** -0.5, 0.09375, ((0, 32), (1, 16))),
    }


def normalize(tokens, norm_gain):
    values = tokens.astype(jnp.float32)
    scale = lax.rsqrt(lax.optimization_barrier(jnp.mean(values * values, axis=-1, keepdims=True)) + 1e-06)
    return (values * scale * norm_gain[None, :]).astype(jnp.bfloat16)

def reference(tokens, norm_gain, chosen, route_weight, gate_weight, up_weight, down_weight):
    normed = normalize(tokens, norm_gain)

    def expert_step(combined, inputs):
        token_ids, weights, gate_mat, up_mat, down_mat = inputs
        expert_rows = normed[token_ids]
        gate_pre = jnp.dot(expert_rows, gate_mat, preferred_element_type=jnp.float32)
        up_pre = jnp.dot(expert_rows, up_mat, preferred_element_type=jnp.float32)
        hidden = (jax.nn.silu(gate_pre) * up_pre).astype(jnp.bfloat16)
        hidden_blocks = hidden.reshape(CAP, N_TP, FF_BLK).astype(jnp.float32)
        down_blocks = down_mat.reshape(N_TP, FF_BLK, D).astype(jnp.float32)
        partial_value = jnp.einsum('cnf,nfd->ncd', hidden_blocks, down_blocks).astype(jnp.bfloat16)
        partial_value = lax.optimization_barrier(partial_value)
        summed = lax.optimization_barrier(jnp.sum(partial_value.astype(jnp.float32), axis=0))
        weighted = (weights[:, None] * summed).astype(jnp.bfloat16)
        combined = combined.at[token_ids].add(weighted.astype(jnp.float32))
        return (combined, None)
    start_total = jnp.zeros((TOKENS, D), jnp.float32)
    combined, _ = lax.scan(expert_step, start_total, (chosen, route_weight, gate_weight, up_weight, down_weight))
    return combined.astype(jnp.bfloat16)
```

```python
import functools

import jax
import jax.numpy as jnp
from jax import lax
from jax.experimental import pallas as pl
from jax.experimental.pallas import tpu as pltpu
from jax.sharding import Mesh
from jax.sharding import PartitionSpec as P

NZ, NX, NY, NC = 8, 4, 8, 2
EP = NZ * NX
BF = jnp.bfloat16
F32 = jnp.float32
LANES = 128
COPY = pltpu.make_async_copy


def remote(src, dst, send, recv, where):
    return pltpu.make_async_remote_copy(
        src_ref=src, dst_ref=dst, send_sem=send, recv_sem=recv,
        device_id=where, device_id_type=pl.DeviceIdType.MESH,
    )


def hops_of(way, half):
    return NY // 2 if way == half else NY // 2 - 1


def kernel(
    slots, tokens, gain, slot_tok, flat, rw, gate, up, down, out,
    tok_v, gu_v, dw_v, place, unpack, sendbuf, recvbuf, ag, acc, hidden, part, rs_first, rs, back, ret,
    tok_sem, w_sem, wx_send, wx_recv, ep_send, ep_recv, ag_send, ag_recv, rs_send, rs_recv, ret_send, ret_recv,
):
    z, x = lax.axis_index("z"), lax.axis_index("x")
    y, c = lax.axis_index("y"), lax.axis_index("c")
    block = z * NX + x
    rows = ag.shape[2]
    width = 2 * LANES
    ff = gate.shape[1]
    model = tokens.shape[1]
    half_slots = EP * slots

    def wrap(v):
        return lax.rem(v + NY, NY)

    def chip(index, core):
        return (index // NX, lax.rem(index, NX), y, core)

    def along(way):
        return (z, x, wrap(y + 1) if way == 0 else wrap(y - 1), c)

    tok_copy = COPY(tokens, tok_v, tok_sem)
    tok_copy.start()
    own = [
        COPY(gate, gu_v.at[:, pl.ds(0, ff)], w_sem.at[0]),
        COPY(up, gu_v.at[:, pl.ds(ff, ff)], w_sem.at[1]),
        COPY(down, dw_v.at[pl.ds(0, ff), :], w_sem.at[2]),
    ]
    for copy in own:
        copy.start()

    barrier = pltpu.get_barrier_semaphore()
    plane = EP * NC
    me = block * NC + c

    def greet(i, _):
        other = lax.rem(me + i, plane)
        pl.semaphore_signal(
            barrier, inc=1, device_id=chip(other // NC, lax.rem(other, NC)),
            device_id_type=pl.DeviceIdType.MESH,
        )
        return 0

    for way in range(2):
        pl.semaphore_signal(barrier, inc=1, device_id=along(way), device_id_type=pl.DeviceIdType.MESH)
    lax.fori_loop(1, plane, greet, 0)

    token_ids = lax.broadcasted_iota(jnp.int32, (tok_v.shape[0], half_slots), 0)
    for rel in range(2):
        at = pl.ds(rel * half_slots, half_slots)
        place[:, at] = jnp.where(token_ids == slot_tok[:, at], 1.0, 0.0).astype(BF)

    tok_copy.wait()
    squares = jnp.zeros((tok_v.shape[0], 1), F32)
    for part_at in range(0, model, 512):
        values = tok_v[:, pl.ds(part_at, 512)].astype(F32)
        squares = squares + jnp.sum(values * values, axis=-1, keepdims=True)
    scale = lax.rsqrt(squares / model + 1e-06)
    columns = pl.ds(pl.multiple_of(y * width, width), width)
    normed = (tok_v[:, columns].astype(F32) * scale * gain[:, columns]).astype(BF)
    packed = lax.dot_general(
        place[:, pl.ds(0, half_slots)], normed, (((0,), (0,)), ((), ())), preferred_element_type=F32
    )
    for h in range(2):
        sendbuf[h] = packed[:, h * LANES:(h + 1) * LANES].astype(BF).reshape(EP, slots, LANES)

    pl.semaphore_wait(barrier, plane - 1 + 2)

    for h in range(2):
        COPY(sendbuf.at[h, block], recvbuf.at[h, block], ep_recv.at[h]).start()

        def exchange(i, _):
            other = lax.rem(block + i, EP)
            remote(
                sendbuf.at[h, other], recvbuf.at[h, block], ep_send.at[h], ep_recv.at[h], chip(other, c)
            ).start()
            return 0

        lax.fori_loop(1, EP, exchange, 0)

    sibling = (z, x, y, 1 - c)
    shared = [
        remote(gate, gu_v.at[:, pl.ds(2 * ff, ff)], wx_send.at[0], wx_recv.at[0], sibling),
        remote(up, gu_v.at[:, pl.ds(3 * ff, ff)], wx_send.at[1], wx_recv.at[1], sibling),
        remote(down, dw_v.at[pl.ds(ff, ff), :], wx_send.at[2], wx_recv.at[2], sibling),
    ]
    for copy in shared:
        copy.start()

    slot_ids = lax.broadcasted_iota(jnp.int32, (half_slots, rows), 0)
    unpack[...] = jnp.where(slot_ids == flat[...], 1.0, 0.0).astype(BF)

    def ag_copy(way, h, hop):
        source = wrap(y - hop + 1) if way == 0 else wrap(y + hop - 1)
        where = ag.at[h, source]
        return remote(where, where, ag_send.at[way, h, hop - 1], ag_recv.at[way, h, hop - 1], along(way))

    for h in range(2):
        COPY(recvbuf.at[h], recvbuf.at[h], ep_recv.at[h]).wait()
        ag[h, y] = lax.dot_general(
            unpack[...], recvbuf[h].reshape(half_slots, LANES), (((0,), (0,)), ((), ())),
            preferred_element_type=F32,
        ).astype(BF)
        for way in range(2):
            ag_copy(way, h, 1).start()

    for copy in own:
        copy.wait()
    for copy in shared[:2]:
        copy.wait_recv()

    def gather_in(source, first):
        x_rows = jnp.concatenate([ag[0, source], ag[1, source]], axis=1)
        k_at = pl.ds(pl.multiple_of(source * width, width), width)

        def tile(n, _):
            n_at = pl.ds(pl.multiple_of(n * ff, ff), ff)
            product = jnp.dot(x_rows, gu_v[k_at, n_at], preferred_element_type=F32)
            if first:
                acc[:, n_at] = product
            else:
                acc[:, n_at] += product
            return 0

        lax.fori_loop(0, 4, tile, 0)

    gather_in(y, True)
    for hop in range(1, NY // 2 + 1):
        for h in range(2):
            for way in range(2):
                if hop <= hops_of(way, h):
                    ag_copy(way, h, hop).wait_recv()
                    if hop < hops_of(way, h):
                        ag_copy(way, h, hop + 1).start()
        gather_in(wrap(y - hop), False)
        if hop < NY // 2:
            gather_in(wrap(y + hop), False)

    for s in range(2):
        gate_pre = acc[:, pl.ds(2 * s * ff, ff)]
        up_pre = acc[:, pl.ds((2 * s + 1) * ff, ff)]
        hidden[:, pl.ds(s * ff, ff)] = (gate_pre / (1.0 + jnp.exp(-gate_pre)) * up_pre).astype(BF)
    shared[2].wait_recv()

    def partial_of(offset):
        target = wrap(y + offset)
        return jnp.dot(
            hidden[...], dw_v[:, pl.ds(pl.multiple_of(target * width, width), width)],
            preferred_element_type=F32,
        )

    def rs_copy(way, h, hop):
        source = rs_first.at[way, h] if hop == 1 else rs.at[way, h, hop - 2]
        return remote(
            source, rs.at[way, h, hop - 1], rs_send.at[way, h, hop - 1], rs_recv.at[way, h, hop - 1], along(way)
        )

    far = NY // 2
    product = partial_of(far)
    for way in range(2):
        h = way
        rs_first[way, h] = product[:, h * LANES:(h + 1) * LANES].astype(BF)
        rs_copy(way, h, 1).start()
    for way in range(2):
        h = 1 - way
        offset = far - 1 if way == 0 else 1 - far
        product = partial_of(offset)
        rs_first[way, h] = product[:, h * LANES:(h + 1) * LANES].astype(BF)
        rs_copy(way, h, 1).start()
        part[offset % NY] = product
    for offset in (2, -2, 1, -1, 0):
        part[offset % NY] = partial_of(offset)

    for hop in range(1, far):
        for order in range(2):
            for way in range(2):
                h = way if order == 0 else 1 - way
                hops = hops_of(way, h)
                if hop < hops:
                    rs_copy(way, h, hop).wait_recv()
                    offset = hops - hop if way == 0 else hop - hops
                    mine = part[offset % NY, :, pl.ds(h * LANES, LANES)]
                    rs[way, h, hop - 1] = (rs[way, h, hop - 1].astype(F32) + mine).astype(BF)
                    rs_copy(way, h, hop + 1).start()

    factor = jnp.broadcast_to(rw[...], (LANES, rows)).T
    for h in range(2):
        for way in range(2):
            rs_copy(way, h, hops_of(way, h)).wait_recv()
        total = part[0, :, pl.ds(h * LANES, LANES)]
        for way in range(2):
            total = total + rs[way, h, hops_of(way, h) - 1].astype(F32)
        weighted = (total * factor).astype(BF)
        back[h] = (
            jnp.dot(unpack[...], weighted, preferred_element_type=F32).astype(BF).reshape(EP, slots, LANES)
        )
        rel = lax.rem(c + h, 2)

        def give(i, _):
            other = lax.rem(block + i, EP)
            remote(back.at[h, other], ret.at[rel, block], ret_send, ret_recv, chip(other, h)).start()
            return 0

        lax.fori_loop(1, EP, give, 0)

        @pl.when(c == h)
        def _():
            COPY(back.at[h, block], ret.at[rel, block], ret_recv).start()

        @pl.when(c != h)
        def _():
            remote(back.at[h, block], ret.at[rel, block], ret_send, ret_recv, chip(block, h)).start()

    COPY(ret, ret, ret_recv).wait()
    out[...] = jnp.dot(
        place[...], ret[...].reshape(2 * half_slots, LANES), preferred_element_type=F32
    ).astype(BF)

    for h in range(2):
        sent = sendbuf.at[h, pl.ds(0, EP - 1)]
        COPY(sent, sent, ep_send.at[h]).wait()
        for way in range(2):
            for hop in range(1, hops_of(way, h) + 1):
                ag_copy(way, h, hop).wait_send()
                rs_copy(way, h, hop).wait_send()
    for copy in shared:
        copy.wait_send()
    for h in range(2):
        sent = back.at[h, pl.ds(0, EP - h)]
        COPY(sent, sent, ret_send).wait()


def shards(tokens, norm_gain, chosen, route_weight, gate_weight, up_weight, down_weight):
    tok_rows, model = tokens.shape
    experts, capacity = chosen.shape
    ff = gate_weight.shape[2]
    slots = 3 * tok_rows // 32
    rows = capacity // 2
    block = lax.axis_index(("z", "x"))
    c = lax.axis_index("c")

    first = block * tok_rows
    start = jnp.sum((chosen < first).astype(jnp.int32), axis=1)
    end = jnp.sum((chosen < first + tok_rows).astype(jnp.int32), axis=1)
    parity = (c + jnp.arange(2, dtype=jnp.int32)) & 1
    lead = start[None, :] + ((start[None, :] + parity[:, None]) & 1)
    position = lead[:, :, None] + 2 * jnp.arange(slots, dtype=jnp.int32)[None, None, :]
    hit = position[:, :, :, None] == jnp.arange(capacity, dtype=jnp.int32)
    token = jnp.sum(jnp.where(hit, chosen[None, :, None, :] - first, 0), axis=-1)
    slot_tok = jnp.where(position < end[None, :, None], token, -1).reshape(1, -1)

    def mine(row):
        return lax.dynamic_index_in_dim(row.reshape(rows, 2), c, 1, keepdims=False)

    source = mine(lax.dynamic_index_in_dim(chosen, block, 0, keepdims=False)) // tok_rows
    before = jnp.sum((source[:, None] < source[None, :]).astype(jnp.int32), axis=0)
    flat = (source * slots + jnp.arange(rows, dtype=jnp.int32) - before).reshape(1, rows)
    rw = mine(route_weight[0]).reshape(1, rows)

    vmem = pl.BlockSpec(memory_space=pltpu.VMEM)
    hbm = pl.BlockSpec(memory_space=pl.ANY)
    far = NY // 2
    dma = pltpu.SemaphoreType.DMA
    return pl.pallas_call(
        functools.partial(kernel, slots),
        out_shape=jax.ShapeDtypeStruct((tok_rows, model // (NY * NC)), BF),
        in_specs=[hbm, vmem, vmem, vmem, vmem, hbm, hbm, hbm],
        out_specs=vmem,
        scratch_shapes=[
            pltpu.VMEM((tok_rows, model), BF),
            pltpu.VMEM((model, 4 * ff), BF),
            pltpu.VMEM((2 * ff, model), BF),
            pltpu.VMEM((tok_rows, 2 * EP * slots), BF),
            pltpu.VMEM((EP * slots, rows), BF),
            pltpu.VMEM((2, EP, slots, LANES), BF),
            pltpu.VMEM((2, EP, slots, LANES), BF),
            pltpu.VMEM((2, NY, rows, LANES), BF),
            pltpu.VMEM((rows, 4 * ff), F32),
            pltpu.VMEM((rows, 2 * ff), BF),
            pltpu.VMEM((NY, rows, 2 * LANES), F32),
            pltpu.VMEM((2, 2, rows, LANES), BF),
            pltpu.VMEM((2, 2, far, rows, LANES), BF),
            pltpu.VMEM((2, EP, slots, LANES), BF),
            pltpu.VMEM((2, EP, slots, LANES), BF),
            dma(()),
            dma((3,)),
            dma((3,)),
            dma((3,)),
            dma((2,)),
            dma((2,)),
            dma((2, 2, far)),
            dma((2, 2, far)),
            dma((2, 2, far)),
            dma((2, 2, far)),
            dma(()),
            dma(()),
        ],
        compiler_params=pltpu.CompilerParams(
            collective_id=0, has_side_effects=True, vmem_limit_bytes=56 * 1024 * 1024
        ),
    )(tokens, norm_gain.reshape(1, -1), slot_tok, flat, rw, gate_weight[0], up_weight[0], down_weight[0])


def solution(mesh):
    finer = Mesh(mesh.devices.reshape(NZ, NX, NY, NC), ("z", "x", "y", "c"))
    ep, tp = ("z", "x"), ("y", "c")
    in_specs = (
        P(ep, None),
        P(),
        P(),
        P(ep, None),
        P(ep, None, tp),
        P(ep, None, tp),
        P(ep, tp, None),
    )
    return jax.shard_map(
        shards, mesh=finer, in_specs=in_specs, out_specs=P(ep, tp), check_vma=False
    )
```

```python
import functools

import jax
import jax.numpy as jnp
from jax import lax
from jax.experimental import pallas as pl
from jax.experimental.pallas import tpu as pltpu
from jax.sharding import Mesh
from jax.sharding import PartitionSpec as P

NZ, NX, NY, NC = 8, 4, 8, 2
EP = NZ * NX
BF = jnp.bfloat16
F32 = jnp.float32
LANES = 128
COPY = pltpu.make_async_copy


def remote(src, dst, send, recv, where):
    return pltpu.make_async_remote_copy(
        src_ref=src, dst_ref=dst, send_sem=send, recv_sem=recv,
        device_id=where, device_id_type=pl.DeviceIdType.MESH,
    )


def hops_of(way, half):
    return NY // 2 if way == half else NY // 2 - 1


def kernel(
    slots, tokens, gain, chosen, rw, gate, up, down, out,
    tok_v, gu_v, dw_v, values, dist, rank, factor, place, place_t, unpack, unpack_t, sendbuf, recvbuf, ag, acc, hidden, part, rs_first, rs, back, ret,
    tok_sem, w_sem, wx_send, wx_recv, ep_send, ep_recv, ag_send, ag_recv, rs_send, rs_recv, ret_send, ret_recv,
):
    z, x = lax.axis_index("z"), lax.axis_index("x")
    y, c = lax.axis_index("y"), lax.axis_index("c")
    block = z * NX + x
    rows = ag.shape[2]
    width = 2 * LANES
    ff = gate.shape[1]
    model = tokens.shape[1]
    half_slots = EP * slots

    def wrap(v):
        return lax.rem(v + NY, NY)

    def chip(index, core):
        return (index // NX, lax.rem(index, NX), y, core)

    def along(way):
        return (z, x, wrap(y + 1) if way == 0 else wrap(y - 1), c)

    tok_copy = COPY(tokens, tok_v, tok_sem)
    tok_copy.start()
    own = [
        COPY(gate, gu_v.at[:, pl.ds(0, ff)], w_sem.at[0]),
        COPY(up, gu_v.at[:, pl.ds(ff, ff)], w_sem.at[1]),
        COPY(down, dw_v.at[pl.ds(0, ff), :], w_sem.at[2]),
    ]
    for copy in own:
        copy.start()

    barrier = pltpu.get_barrier_semaphore()
    plane = EP * NC
    me = block * NC + c

    def greet(i, _):
        other = lax.rem(me + i, plane)
        pl.semaphore_signal(
            barrier, inc=1, device_id=chip(other // NC, lax.rem(other, NC)),
            device_id_type=pl.DeviceIdType.MESH,
        )
        return 0

    for way in range(2):
        pl.semaphore_signal(barrier, inc=1, device_id=along(way), device_id_type=pl.DeviceIdType.MESH)
    lax.fori_loop(1, plane, greet, 0)

    tok_rows, capacity = tok_v.shape[0], chosen.shape[1]
    first = block * tok_rows
    pair = 2 * slots
    slot_steps = lax.broadcasted_iota(jnp.int32, (slots, 1), 0)
    positions = lax.broadcasted_iota(jnp.int32, (1, capacity), 1)

    def count(hits):
        return jnp.sum(jnp.where(hits, 1.0, 0.0), axis=1, keepdims=True).astype(jnp.int32)

    run_start = count(chosen[...] < first)
    values[...] = (chosen[...] - (first - 1)).astype(F32)
    token_ids = (lax.broadcasted_iota(jnp.int32, (1, tok_rows), 1) + 1).astype(F32)

    def build_place(rel):
        parity = lax.rem(c + rel, 2)
        lead = run_start + ((run_start + parity) & 1)
        dist[...] = positions - lead

        def body(i, _):
            made = []
            for k in range(2):
                at = pl.ds(2 * i + k, 1)
                found = jnp.where(dist[at, :] == 2 * slot_steps, values[at, :], 0.0)
                token = jnp.sum(found, axis=1, keepdims=True)
                made.append(jnp.where(token == token_ids, 1.0, 0.0))
            to = pl.ds(pl.multiple_of(rel * half_slots + i * pair, pair), pair)
            place[to, :] = jnp.concatenate(made, axis=0).astype(BF)
            return 0

        lax.fori_loop(0, EP // 2, body, 0, unroll=4)

    def build_unpack():
        edges = lax.broadcasted_iota(jnp.int32, (EP, 1), 0) * tok_rows
        row = chosen[pl.ds(block, 1), :]
        lo, hi = count(row < edges), count(row < edges + tok_rows)
        lead = lo + ((lo + c) & 1)
        base = (lead - c) >> 1
        filled = (hi - lead + 1) >> 1
        ahead = lax.broadcasted_iota(jnp.int32, (1, rows), 1) - base
        rank[...] = jnp.where((ahead >= 0) & (ahead < filled), ahead, -1)

        def body(i, _):
            made = [
                jnp.where(rank[pl.ds(2 * i + k, 1), :] == slot_steps, 1.0, 0.0) for k in range(2)
            ]
            unpack[pl.ds(pl.multiple_of(i * pair, pair), pair), :] = jnp.concatenate(made, axis=0).astype(BF)
            return 0

        lax.fori_loop(0, EP // 2, body, 0, unroll=4)
        unpack_t[...] = unpack[...].T

    def build_factor():
        step = min(LANES, rows)

        def body(i, _):
            at = pl.ds(pl.multiple_of(i * step, step), step)
            wanted = 2 * (lax.broadcasted_iota(jnp.int32, (step, 1), 0) + i * step) + c
            found = jnp.where(positions == wanted, rw[...], 0.0)
            factor[at, :] = jnp.broadcast_to(jnp.sum(found, axis=1, keepdims=True), (step, LANES))
            return 0

        lax.fori_loop(0, rows // step, body, 0)

    build_place(0)
    tok_copy.wait()
    squares = jnp.zeros((tok_v.shape[0], 1), F32)
    for part_at in range(0, model, 512):
        some = tok_v[:, pl.ds(part_at, 512)].astype(F32)
        squares = squares + jnp.sum(some * some, axis=-1, keepdims=True)
    scale = lax.rsqrt(squares / model + 1e-06)
    columns = pl.ds(pl.multiple_of(y * width, width), width)
    normed = (tok_v[:, columns].astype(F32) * scale * gain[:, columns]).astype(BF)
    packed = jnp.dot(place[pl.ds(0, half_slots), :], normed, preferred_element_type=F32)
    for h in range(2):
        sendbuf[h] = packed[:, h * LANES:(h + 1) * LANES].astype(BF).reshape(EP, slots, LANES)

    pl.semaphore_wait(barrier, plane - 1 + 2)

    for h in range(2):
        COPY(sendbuf.at[h, block], recvbuf.at[h, block], ep_recv.at[h]).start()

        def exchange(i, _):
            other = lax.rem(block + i, EP)
            remote(
                sendbuf.at[h, other], recvbuf.at[h, block], ep_send.at[h], ep_recv.at[h], chip(other, c)
            ).start()
            return 0

        lax.fori_loop(1, EP, exchange, 0)

    sibling = (z, x, y, 1 - c)
    shared = [
        remote(gate, gu_v.at[:, pl.ds(2 * ff, ff)], wx_send.at[0], wx_recv.at[0], sibling),
        remote(up, gu_v.at[:, pl.ds(3 * ff, ff)], wx_send.at[1], wx_recv.at[1], sibling),
        remote(down, dw_v.at[pl.ds(ff, ff), :], wx_send.at[2], wx_recv.at[2], sibling),
    ]
    for copy in shared:
        copy.start()

    build_unpack()

    def ag_copy(way, h, hop):
        source = wrap(y - hop + 1) if way == 0 else wrap(y + hop - 1)
        where = ag.at[h, source]
        return remote(where, where, ag_send.at[way, h, hop - 1], ag_recv.at[way, h, hop - 1], along(way))

    for h in range(2):
        COPY(recvbuf.at[h], recvbuf.at[h], ep_recv.at[h]).wait()
        ag[h, y] = jnp.dot(
            unpack_t[...], recvbuf[h].reshape(half_slots, LANES), preferred_element_type=F32
        ).astype(BF)
        for way in range(2):
            ag_copy(way, h, 1).start()

    for copy in own:
        copy.wait()
    for copy in shared[:2]:
        copy.wait_recv()

    def gather_in(source, first):
        x_rows = jnp.concatenate([ag[0, source], ag[1, source]], axis=1)
        k_at = pl.ds(pl.multiple_of(source * width, width), width)

        def tile(n, _):
            n_at = pl.ds(pl.multiple_of(n * ff, ff), ff)
            product = jnp.dot(x_rows, gu_v[k_at, n_at], preferred_element_type=F32)
            if first:
                acc[:, n_at] = product
            else:
                acc[:, n_at] += product
            return 0

        lax.fori_loop(0, 4, tile, 0)

    gather_in(y, True)
    build_factor()
    build_place(1)
    place_t[...] = place[...].T
    for hop in range(1, NY // 2 + 1):
        for h in range(2):
            for way in range(2):
                if hop <= hops_of(way, h):
                    ag_copy(way, h, hop).wait_recv()
                    if hop < hops_of(way, h):
                        ag_copy(way, h, hop + 1).start()
        gather_in(wrap(y - hop), False)
        if hop < NY // 2:
            gather_in(wrap(y + hop), False)

    for s in range(2):
        gate_pre = acc[:, pl.ds(2 * s * ff, ff)]
        up_pre = acc[:, pl.ds((2 * s + 1) * ff, ff)]
        hidden[:, pl.ds(s * ff, ff)] = (gate_pre / (1.0 + jnp.exp(-gate_pre)) * up_pre).astype(BF)
    shared[2].wait_recv()

    def partial_of(offset):
        target = wrap(y + offset)
        return jnp.dot(
            hidden[...], dw_v[:, pl.ds(pl.multiple_of(target * width, width), width)],
            preferred_element_type=F32,
        )

    def rs_copy(way, h, hop):
        source = rs_first.at[way, h] if hop == 1 else rs.at[way, h, hop - 2]
        return remote(
            source, rs.at[way, h, hop - 1], rs_send.at[way, h, hop - 1], rs_recv.at[way, h, hop - 1], along(way)
        )

    far = NY // 2
    product = partial_of(far)
    for way in range(2):
        h = way
        rs_first[way, h] = product[:, h * LANES:(h + 1) * LANES].astype(BF)
        rs_copy(way, h, 1).start()
    for way in range(2):
        h = 1 - way
        offset = far - 1 if way == 0 else 1 - far
        product = partial_of(offset)
        rs_first[way, h] = product[:, h * LANES:(h + 1) * LANES].astype(BF)
        rs_copy(way, h, 1).start()
        part[offset % NY] = product
    for offset in (2, -2, 1, -1, 0):
        part[offset % NY] = partial_of(offset)

    for hop in range(1, far):
        for order in range(2):
            for way in range(2):
                h = way if order == 0 else 1 - way
                hops = hops_of(way, h)
                if hop < hops:
                    rs_copy(way, h, hop).wait_recv()
                    offset = hops - hop if way == 0 else hop - hops
                    mine = part[offset % NY, :, pl.ds(h * LANES, LANES)]
                    rs[way, h, hop - 1] = (rs[way, h, hop - 1].astype(F32) + mine).astype(BF)
                    rs_copy(way, h, hop + 1).start()

    for h in range(2):
        for way in range(2):
            rs_copy(way, h, hops_of(way, h)).wait_recv()
        total = part[0, :, pl.ds(h * LANES, LANES)]
        for way in range(2):
            total = total + rs[way, h, hops_of(way, h) - 1].astype(F32)
        weighted = (total * factor[...]).astype(BF)
        back[h] = (
            jnp.dot(unpack[...], weighted, preferred_element_type=F32).astype(BF).reshape(EP, slots, LANES)
        )
        rel = lax.rem(c + h, 2)

        def give(i, _):
            other = lax.rem(block + i, EP)
            remote(back.at[h, other], ret.at[rel, block], ret_send, ret_recv, chip(other, h)).start()
            return 0

        lax.fori_loop(1, EP, give, 0)

        @pl.when(c == h)
        def _():
            COPY(back.at[h, block], ret.at[rel, block], ret_recv).start()

        @pl.when(c != h)
        def _():
            remote(back.at[h, block], ret.at[rel, block], ret_send, ret_recv, chip(block, h)).start()

    COPY(ret, ret, ret_recv).wait()
    out[...] = jnp.dot(
        place_t[...], ret[...].reshape(2 * half_slots, LANES), preferred_element_type=F32
    ).astype(BF)

    for h in range(2):
        sent = sendbuf.at[h, pl.ds(0, EP - 1)]
        COPY(sent, sent, ep_send.at[h]).wait()
        for way in range(2):
            for hop in range(1, hops_of(way, h) + 1):
                ag_copy(way, h, hop).wait_send()
                rs_copy(way, h, hop).wait_send()
    for copy in shared:
        copy.wait_send()
    for h in range(2):
        sent = back.at[h, pl.ds(0, EP - h)]
        COPY(sent, sent, ret_send).wait()


def shards(tokens, norm_gain, chosen, route_weight, gate_weight, up_weight, down_weight):
    tok_rows, model = tokens.shape
    experts, capacity = chosen.shape
    ff = gate_weight.shape[2]
    slots = 3 * tok_rows // 32
    rows = capacity // 2
    vmem = pl.BlockSpec(memory_space=pltpu.VMEM)
    hbm = pl.BlockSpec(memory_space=pl.ANY)
    far = NY // 2
    dma = pltpu.SemaphoreType.DMA
    return pl.pallas_call(
        functools.partial(kernel, slots),
        out_shape=jax.ShapeDtypeStruct((tok_rows, model // (NY * NC)), BF),
        in_specs=[hbm, vmem, vmem, vmem, hbm, hbm, hbm],
        out_specs=vmem,
        scratch_shapes=[
            pltpu.VMEM((tok_rows, model), BF),
            pltpu.VMEM((model, 4 * ff), BF),
            pltpu.VMEM((2 * ff, model), BF),
            pltpu.VMEM((experts, capacity), F32),
            pltpu.VMEM((experts, capacity), jnp.int32),
            pltpu.VMEM((EP, rows), jnp.int32),
            pltpu.VMEM((rows, LANES), F32),
            pltpu.VMEM((2 * EP * slots, tok_rows), BF),
            pltpu.VMEM((tok_rows, 2 * EP * slots), BF),
            pltpu.VMEM((EP * slots, rows), BF),
            pltpu.VMEM((rows, EP * slots), BF),
            pltpu.VMEM((2, EP, slots, LANES), BF),
            pltpu.VMEM((2, EP, slots, LANES), BF),
            pltpu.VMEM((2, NY, rows, LANES), BF),
            pltpu.VMEM((rows, 4 * ff), F32),
            pltpu.VMEM((rows, 2 * ff), BF),
            pltpu.VMEM((NY, rows, 2 * LANES), F32),
            pltpu.VMEM((2, 2, rows, LANES), BF),
            pltpu.VMEM((2, 2, far, rows, LANES), BF),
            pltpu.VMEM((2, EP, slots, LANES), BF),
            pltpu.VMEM((2, EP, slots, LANES), BF),
            dma(()),
            dma((3,)),
            dma((3,)),
            dma((3,)),
            dma((2,)),
            dma((2,)),
            dma((2, 2, far)),
            dma((2, 2, far)),
            dma((2, 2, far)),
            dma((2, 2, far)),
            dma(()),
            dma(()),
        ],
        compiler_params=pltpu.CompilerParams(
            collective_id=0, has_side_effects=True, vmem_limit_bytes=56 * 1024 * 1024
        ),
    )(tokens, norm_gain.reshape(1, -1), chosen, route_weight, gate_weight[0], up_weight[0], down_weight[0])


def solution(mesh):
    finer = Mesh(mesh.devices.reshape(NZ, NX, NY, NC), ("z", "x", "y", "c"))
    ep, tp = ("z", "x"), ("y", "c")
    in_specs = (
        P(ep, None),
        P(),
        P(),
        P(ep, None),
        P(ep, None, tp),
        P(ep, None, tp),
        P(ep, tp, None),
    )
    return jax.shard_map(
        shards, mesh=finer, in_specs=in_specs, out_specs=P(ep, tp), check_vma=False
    )
```

```python
import functools

import jax
import jax.numpy as jnp
from jax import lax
from jax.experimental import pallas as pl
from jax.experimental.pallas import tpu as pltpu
from jax.sharding import Mesh
from jax.sharding import PartitionSpec as P

NZ, NX, NY, NC = 8, 4, 8, 2
EP = NZ * NX
BF = jnp.bfloat16
F32 = jnp.float32
LANES = 128
COPY = pltpu.make_async_copy


def remote(src, dst, send, recv, where):
    return pltpu.make_async_remote_copy(
        src_ref=src, dst_ref=dst, send_sem=send, recv_sem=recv,
        device_id=where, device_id_type=pl.DeviceIdType.MESH,
    )


FAR = NY // 2


def kernel(
    slots, tokens, gain_in, chosen_in, rw_in, gate, up, down, out,
    tok_v, gain, chosen, rw, gu_v, dw_v, values, dist, rank, factor, place, place_t, unpack, unpack_t, sendbuf, recvbuf, ag, acc, hidden, part, rs_first, rs, back, ret,
    tok_sem, in_sem, w_sem, wx_send, wx_recv, ep_send, ep_recv, ag_send, ag_recv, rs_send, rs_recv, ret_send, ret_recv,
):
    z, x = lax.axis_index("z"), lax.axis_index("x")
    y, c = lax.axis_index("y"), lax.axis_index("c")
    block = z * NX + x
    rows = ag.shape[2]
    width = 2 * LANES
    ff = gate.shape[1]
    model = tokens.shape[1]
    half_slots = EP * slots

    def wrap(v):
        return lax.rem(v + NY, NY)

    def chip(index, core):
        return (index // NX, lax.rem(index, NX), y, core)

    def along(way):
        return (z, x, wrap(y + 1) if way == 0 else wrap(y - 1), c)

    small = [
        COPY(chosen_in, chosen, in_sem.at[0]),
        COPY(gain_in, gain, in_sem.at[1]),
        COPY(rw_in, rw, in_sem.at[2]),
    ]
    small[0].start()
    tok_copy = COPY(tokens, tok_v, tok_sem)
    tok_copy.start()
    for copy in small[1:]:
        copy.start()
    own = [
        COPY(gate, gu_v.at[:, pl.ds(0, ff)], w_sem.at[0]),
        COPY(up, gu_v.at[:, pl.ds(ff, ff)], w_sem.at[1]),
        COPY(down, dw_v.at[pl.ds(0, ff), :], w_sem.at[2]),
    ]
    for copy in own:
        copy.start()

    def peer(i):
        k, r = (i - 1) // NX, lax.rem(i - 1, NX)
        away = NZ // 2 - (k + 1) // 2
        dz = jnp.where(lax.rem(k, 2) == 0, NZ - away, away)
        return lax.rem(z + dz, NZ) * NX + lax.rem(x + NX - 1 - r, NX)

    barrier = pltpu.get_barrier_semaphore()
    plane = EP * NC
    me = block * NC + c

    def greet(i, _):
        other = lax.rem(me + i, plane)
        pl.semaphore_signal(
            barrier, inc=1, device_id=chip(other // NC, lax.rem(other, NC)),
            device_id_type=pl.DeviceIdType.MESH,
        )
        return 0

    for way in range(2):
        pl.semaphore_signal(barrier, inc=1, device_id=along(way), device_id_type=pl.DeviceIdType.MESH)
    lax.fori_loop(1, plane, greet, 0)

    tok_rows, capacity = tok_v.shape[0], chosen.shape[1]
    first = block * tok_rows
    pair = 2 * slots
    slot_steps = lax.broadcasted_iota(jnp.int32, (slots, 1), 0)
    positions = lax.broadcasted_iota(jnp.int32, (1, capacity), 1)

    def count(hits):
        return jnp.sum(jnp.where(hits, 1.0, 0.0), axis=1, keepdims=True).astype(jnp.int32)

    small[0].wait()
    run_start = count(chosen[...] < first)
    values[...] = (chosen[...] - (first - 1)).astype(F32)
    token_ids = (lax.broadcasted_iota(jnp.int32, (1, tok_rows), 1) + 1).astype(F32)

    def build_place(rel):
        parity = lax.rem(c + rel, 2)
        lead = run_start + ((run_start + parity) & 1)
        dist[...] = positions - lead

        def body(i, _):
            made = []
            for k in range(2):
                at = pl.ds(2 * i + k, 1)
                found = jnp.where(dist[at, :] == 2 * slot_steps, values[at, :], 0.0)
                token = jnp.sum(found, axis=1, keepdims=True)
                made.append(jnp.where(token == token_ids, 1.0, 0.0))
            to = pl.ds(pl.multiple_of(rel * half_slots + i * pair, pair), pair)
            place[to, :] = jnp.concatenate(made, axis=0).astype(BF)
            return 0

        lax.fori_loop(0, EP // 2, body, 0, unroll=4)

    def build_unpack():
        edges = lax.broadcasted_iota(jnp.int32, (EP, 1), 0) * tok_rows
        row = chosen[pl.ds(block, 1), :]
        lo, hi = count(row < edges), count(row < edges + tok_rows)
        lead = lo + ((lo + c) & 1)
        base = (lead - c) >> 1
        filled = (hi - lead + 1) >> 1
        ahead = lax.broadcasted_iota(jnp.int32, (1, rows), 1) - base
        rank[...] = jnp.where((ahead >= 0) & (ahead < filled), ahead, -1)

        def body(i, _):
            made = [
                jnp.where(rank[pl.ds(2 * i + k, 1), :] == slot_steps, 1.0, 0.0) for k in range(2)
            ]
            unpack[pl.ds(pl.multiple_of(i * pair, pair), pair), :] = jnp.concatenate(made, axis=0).astype(BF)
            return 0

        lax.fori_loop(0, EP // 2, body, 0, unroll=4)
        unpack_t[...] = unpack[...].T

    def build_factor():
        step = min(LANES, rows)

        def body(i, _):
            at = pl.ds(pl.multiple_of(i * step, step), step)
            wanted = 2 * (lax.broadcasted_iota(jnp.int32, (step, 1), 0) + i * step) + c
            found = jnp.where(positions == wanted, rw[...], 0.0)
            factor[at, :] = jnp.broadcast_to(jnp.sum(found, axis=1, keepdims=True), (step, LANES))
            return 0

        lax.fori_loop(0, rows // step, body, 0)

    build_place(0)
    tok_copy.wait()
    for copy in small[1:]:
        copy.wait()
    squares = jnp.zeros((tok_v.shape[0], 1), F32)
    for part_at in range(0, model, 512):
        some = tok_v[:, pl.ds(part_at, 512)].astype(F32)
        squares = squares + jnp.sum(some * some, axis=-1, keepdims=True)
    scale = lax.rsqrt(squares / model + 1e-06)
    normed = []
    for ahead in (0, FAR):
        columns = pl.ds(pl.multiple_of(wrap(y + ahead) * width, width), width)
        normed.append((tok_v[:, columns].astype(F32) * scale * gain[:, columns]).astype(BF))

    def pack(some, q):
        packed = jnp.dot(place[pl.ds(0, half_slots), :], some, preferred_element_type=F32)
        for h in range(2):
            sendbuf[q + h] = packed[:, h * LANES:(h + 1) * LANES].astype(BF).reshape(EP, slots, LANES)

    def exchange(q):
        def body(i, _):
            other = peer(i)
            remote(
                sendbuf.at[q, other], recvbuf.at[q, block], ep_send.at[q], ep_recv.at[q], chip(other, c)
            ).start()
            return 0

        lax.fori_loop(1, EP, body, 0)
        COPY(sendbuf.at[q, block], recvbuf.at[q, block], ep_recv.at[q]).start()

    pack(normed[0], 0)
    pl.semaphore_wait(barrier, plane - 1 + 2)
    exchange(0)
    exchange(1)
    pack(normed[1], 2)

    sibling = (z, x, y, 1 - c)
    shared = [
        remote(gate, gu_v.at[:, pl.ds(2 * ff, ff)], wx_send.at[0], wx_recv.at[0], sibling),
        remote(up, gu_v.at[:, pl.ds(3 * ff, ff)], wx_send.at[1], wx_recv.at[1], sibling),
        remote(down, dw_v.at[pl.ds(ff, ff), :], wx_send.at[2], wx_recv.at[2], sibling),
    ]
    for copy in shared:
        copy.start()
    exchange(2)
    exchange(3)
    build_unpack()

    def ag_copy(way, u, h):
        source = wrap(y + ((0, -1, FAR) if way == 0 else (0, 1, FAR))[u])
        where = ag.at[h, source]
        return remote(where, where, ag_send.at[way, u, h], ag_recv.at[way, u, h], along(way))

    def compact(q):
        COPY(recvbuf.at[q], recvbuf.at[q], ep_recv.at[q]).wait()
        u, h = q // 2, q % 2
        ag[h, wrap(y + u * FAR)] = jnp.dot(
            unpack_t[...], recvbuf[q].reshape(half_slots, LANES), preferred_element_type=F32
        ).astype(BF)
        for way in range(2):
            ag_copy(way, 2 * u, h).start()

    def gather_in(parts, begin=False):
        x_rows = jnp.concatenate([ag[h, source] for h, source in parts], axis=1)

        def tile(n, _):
            n_at = pl.ds(pl.multiple_of(n * ff, ff), ff)
            weight = jnp.concatenate(
                [gu_v[pl.ds(pl.multiple_of(source * width + h * LANES, LANES), LANES), n_at] for h, source in parts],
                axis=0,
            )
            product = jnp.dot(x_rows, weight, preferred_element_type=F32)
            if begin:
                acc[:, n_at] = product
            else:
                acc[:, n_at] += product
            return 0

        lax.fori_loop(0, 4, tile, 0)

    def whole(offset):
        source = wrap(y + offset)
        return [(0, source), (1, source)]

    compact(0)
    build_factor()
    build_place(1)
    place_t[...] = place[...].T
    compact(1)
    for copy in own:
        copy.wait()
    for copy in shared[:2]:
        copy.wait_recv()
    gather_in(whole(0), True)
    for h in range(2):
        for way in range(2):
            ag_copy(way, 0, h).wait_recv()
            ag_copy(way, 1, h).start()
    for offset in (-1, 1):
        gather_in(whole(offset))
    for q in (2, 3):
        compact(q)
    gather_in(whole(FAR))
    for way in range(2):
        for h in range(2):
            ag_copy(way, 1, h).wait_recv()
        gather_in(whole((-2, 2)[way]))
    for h in range(2):
        for way in range(2):
            ag_copy(way, 2, h).wait_recv()
        gather_in([(h, wrap(y - 1 + FAR)), (h, wrap(y + 1 + FAR))])

    for s in range(2):
        gate_pre = acc[:, pl.ds(2 * s * ff, ff)]
        up_pre = acc[:, pl.ds((2 * s + 1) * ff, ff)]
        hidden[:, pl.ds(s * ff, ff)] = (gate_pre / (1.0 + jnp.exp(-gate_pre)) * up_pre).astype(BF)
    shared[2].wait_recv()

    def terms(offset):
        target = wrap(y + offset)
        part[offset % NY] = jnp.dot(
            hidden[...], dw_v[:, pl.ds(pl.multiple_of(target * width, width), width)],
            preferred_element_type=F32,
        )

    piece = [pl.ds(0, rows // 2), pl.ds(rows // 2, rows // 2)]

    def rs_copy(way, h, hop, s):
        source = rs_first.at[way, h] if hop == 0 else rs.at[way, h, hop - 1, piece[s]]
        return remote(
            source, rs.at[way, h, hop, piece[s]],
            rs_send.at[way, h, hop, s], rs_recv.at[way, h, hop, s], along(way),
        )

    def pass_on(way, h, hop, s):
        ahead = FAR - hop if way == 0 else hop - FAR
        mine = part[ahead % NY, piece[s], pl.ds(h * LANES, LANES)]
        if hop == 0:
            rs_first[way, h] = mine.astype(BF)
        else:
            if hop > 1 or s == way:
                rs_copy(way, h, hop - 1, s).wait_recv()
                mine = mine + rs[way, h, hop - 1, piece[s]].astype(F32)
            rs[way, h, hop - 1, piece[s]] = mine.astype(BF)
        rs_copy(way, h, hop, s).start()

    def each_way(h, hop, chained):
        for way in range(2):
            pass_on(way, h, hop, way if chained else 1 - way)

    def finish(h):
        for way in range(2):
            for s in range(2):
                rs_copy(way, h, FAR - 1, s).wait_recv()
        total = part[0, :, pl.ds(h * LANES, LANES)]
        for way in range(2):
            total = total + rs[way, h, FAR - 1].astype(F32)
        weighted = (total * factor[...]).astype(BF)
        back[h] = (
            jnp.dot(unpack[...], weighted, preferred_element_type=F32).astype(BF).reshape(EP, slots, LANES)
        )
        rel = lax.rem(c + h, 2)

        def give(i, _):
            other = peer(i)
            remote(back.at[h, other], ret.at[rel, block], ret_send, ret_recv, chip(other, h)).start()
            return 0

        lax.fori_loop(1, EP, give, 0)

        @pl.when(c == h)
        def _():
            COPY(back.at[h, block], ret.at[rel, block], ret_recv).start()

        @pl.when(c != h)
        def _():
            remote(back.at[h, block], ret.at[rel, block], ret_send, ret_recv, chip(block, h)).start()

    terms(FAR)
    for h in range(2):
        each_way(h, 0, True)
    for offset in (FAR - 1, 1 - FAR):
        terms(offset)
    for h in range(2):
        each_way(h, 1, False)
    for hop in range(2, FAR):
        for offset in (FAR - hop, hop - FAR):
            terms(offset)
    terms(0)
    for h in range(2):
        each_way(h, 1, True)
    for hop in range(2, FAR):
        for h in range(2):
            for chained in (False, True):
                each_way(h, hop, chained)
    for h in range(2):
        finish(h)

    COPY(ret, ret, ret_recv).wait()
    out[...] = jnp.dot(
        place_t[...], ret[...].reshape(2 * half_slots, LANES), preferred_element_type=F32
    ).astype(BF)

    for q in range(4):
        sent = sendbuf.at[q, pl.ds(0, EP - 1)]
        COPY(sent, sent, ep_send.at[q]).wait()
    for h in range(2):
        for way in range(2):
            for u in range(3):
                ag_copy(way, u, h).wait_send()
            for hop in range(FAR):
                for s in range(2):
                    if hop > 0 or s == way:
                        rs_copy(way, h, hop, s).wait_send()
    for copy in shared:
        copy.wait_send()
    for h in range(2):
        sent = back.at[h, pl.ds(0, EP - h)]
        COPY(sent, sent, ret_send).wait()


def shards(tokens, norm_gain, chosen, route_weight, gate_weight, up_weight, down_weight):
    tok_rows, model = tokens.shape
    experts, capacity = chosen.shape
    ff = gate_weight.shape[2]
    slots = 3 * tok_rows // 32
    rows = capacity // 2
    vmem = pl.BlockSpec(memory_space=pltpu.VMEM)
    hbm = pl.BlockSpec(memory_space=pl.ANY)
    dma = pltpu.SemaphoreType.DMA
    return pl.pallas_call(
        functools.partial(kernel, slots),
        out_shape=jax.ShapeDtypeStruct((tok_rows, model // (NY * NC)), BF),
        in_specs=[hbm] * 7,
        out_specs=vmem,
        scratch_shapes=[
            pltpu.VMEM((tok_rows, model), BF),
            pltpu.VMEM((1, model), F32),
            pltpu.VMEM((experts, capacity), jnp.int32),
            pltpu.VMEM((1, capacity), F32),
            pltpu.VMEM((model, 4 * ff), BF),
            pltpu.VMEM((2 * ff, model), BF),
            pltpu.VMEM((experts, capacity), F32),
            pltpu.VMEM((experts, capacity), jnp.int32),
            pltpu.VMEM((EP, rows), jnp.int32),
            pltpu.VMEM((rows, LANES), F32),
            pltpu.VMEM((2 * EP * slots, tok_rows), BF),
            pltpu.VMEM((tok_rows, 2 * EP * slots), BF),
            pltpu.VMEM((EP * slots, rows), BF),
            pltpu.VMEM((rows, EP * slots), BF),
            pltpu.VMEM((4, EP, slots, LANES), BF),
            pltpu.VMEM((4, EP, slots, LANES), BF),
            pltpu.VMEM((2, NY, rows, LANES), BF),
            pltpu.VMEM((rows, 4 * ff), F32),
            pltpu.VMEM((rows, 2 * ff), BF),
            pltpu.VMEM((NY, rows, 2 * LANES), F32),
            pltpu.VMEM((2, 2, rows // 2, LANES), BF),
            pltpu.VMEM((2, 2, FAR, rows, LANES), BF),
            pltpu.VMEM((2, EP, slots, LANES), BF),
            pltpu.VMEM((2, EP, slots, LANES), BF),
            dma(()),
            dma((3,)),
            dma((3,)),
            dma((3,)),
            dma((3,)),
            dma((4,)),
            dma((4,)),
            dma((2, 3, 2)),
            dma((2, 3, 2)),
            dma((2, 2, FAR, 2)),
            dma((2, 2, FAR, 2)),
            dma(()),
            dma(()),
        ],
        compiler_params=pltpu.CompilerParams(
            collective_id=0, has_side_effects=True, vmem_limit_bytes=56 * 1024 * 1024
        ),
    )(tokens, norm_gain.reshape(1, -1), chosen, route_weight, gate_weight[0], up_weight[0], down_weight[0])


def solution(mesh):
    finer = Mesh(mesh.devices.reshape(NZ, NX, NY, NC), ("z", "x", "y", "c"))
    ep, tp = ("z", "x"), ("y", "c")
    in_specs = (
        P(ep, None),
        P(),
        P(),
        P(ep, None),
        P(ep, None, tp),
        P(ep, None, tp),
        P(ep, tp, None),
    )
    return jax.shard_map(
        shards, mesh=finer, in_specs=in_specs, out_specs=P(ep, tp), check_vma=False
    )
```

```python
import functools

import jax
import jax.numpy as jnp
from jax import lax
from jax.experimental import pallas as pl
from jax.experimental.pallas import tpu as pltpu
from jax.sharding import Mesh
from jax.sharding import PartitionSpec as P

NZ, NX, NY, NC = 8, 4, 8, 2
EP = NZ * NX
BF = jnp.bfloat16
F32 = jnp.float32
LANES = 128
COPY = pltpu.make_async_copy


def remote(src, dst, send, recv, where):
    return pltpu.make_async_remote_copy(
        src_ref=src, dst_ref=dst, send_sem=send, recv_sem=recv,
        device_id=where, device_id_type=pl.DeviceIdType.MESH,
    )


FAR = NY // 2


def kernel(
    slots, tokens, gain_in, chosen_in, rw_in, gate, up, down, out,
    tok_v, gain, chosen, rw, gu_v, dw_v, values, dist, rank, factor, place, place_t, unpack, unpack_t, sendbuf, recvbuf, ag, acc, hidden, part, rs_first, rs, back, ret,
    tok_sem, in_sem, w_sem, wx_send, wx_recv, ep_send, ep_recv, ag_send, ag_recv, rs_send, rs_recv, ret_send, ret_recv,
):
    z, x = lax.axis_index("z"), lax.axis_index("x")
    y, c = lax.axis_index("y"), lax.axis_index("c")
    block = z * NX + x
    rows = ag.shape[2]
    width = 2 * LANES
    ff = gate.shape[1]
    model = tokens.shape[1]
    half_slots = EP * slots

    def wrap(v):
        return lax.rem(v + NY, NY)

    def chip(index, core):
        return (index // NX, lax.rem(index, NX), y, core)

    def along(way):
        return (z, x, wrap(y + 1) if way == 0 else wrap(y - 1), c)

    small = [
        COPY(chosen_in, chosen, in_sem.at[0]),
        COPY(gain_in, gain, in_sem.at[1]),
        COPY(rw_in, rw, in_sem.at[2]),
    ]
    small[0].start()
    tok_copy = COPY(tokens, tok_v, tok_sem)
    tok_copy.start()
    for copy in small[1:]:
        copy.start()
    own = [
        COPY(gate, gu_v.at[:, pl.ds(0, ff)], w_sem.at[0]),
        COPY(up, gu_v.at[:, pl.ds(ff, ff)], w_sem.at[1]),
        COPY(down, dw_v.at[pl.ds(0, ff), :], w_sem.at[2]),
    ]
    for copy in own:
        copy.start()

    def peer(i):
        step = (i + 1) // 2
        return lax.rem(block + jnp.where(lax.rem(i, 2) == 1, step, EP - step), EP)

    barrier = pltpu.get_barrier_semaphore()
    plane = EP * NC
    apart = sorted(range(NZ), key=lambda dz: -min(dz, NZ - dz))
    for dz in apart:
        for dx in range(NX - 1, -1, -1):
            for dc in range(NC):
                if dz or dx or dc:
                    pl.semaphore_signal(
                        barrier, inc=1,
                        device_id=(lax.rem(z + dz, NZ), lax.rem(x + dx, NX), y, lax.rem(c + dc, NC)),
                        device_id_type=pl.DeviceIdType.MESH,
                    )
    for way in range(2):
        pl.semaphore_signal(barrier, inc=1, device_id=along(way), device_id_type=pl.DeviceIdType.MESH)

    tok_rows, capacity = tok_v.shape[0], chosen.shape[1]
    first = block * tok_rows
    pair = 2 * slots
    slot_steps = lax.broadcasted_iota(jnp.int32, (slots, 1), 0)
    positions = lax.broadcasted_iota(jnp.int32, (1, capacity), 1)

    def count(hits):
        return jnp.sum(jnp.where(hits, 1.0, 0.0), axis=1, keepdims=True).astype(jnp.int32)

    small[0].wait()
    run_start = count(chosen[...] < first)
    values[...] = (chosen[...] - (first - 1)).astype(F32)
    token_ids = (lax.broadcasted_iota(jnp.int32, (1, tok_rows), 1) + 1).astype(F32)

    def build_place(rel):
        parity = lax.rem(c + rel, 2)
        lead = run_start + ((run_start + parity) & 1)
        dist[...] = positions - lead

        def body(i, _):
            made = []
            for k in range(2):
                at = pl.ds(2 * i + k, 1)
                found = jnp.where(dist[at, :] == 2 * slot_steps, values[at, :], 0.0)
                token = jnp.sum(found, axis=1, keepdims=True)
                made.append(jnp.where(token == token_ids, 1.0, 0.0))
            to = pl.ds(pl.multiple_of(rel * half_slots + i * pair, pair), pair)
            place[to, :] = jnp.concatenate(made, axis=0).astype(BF)
            return 0

        lax.fori_loop(0, EP // 2, body, 0, unroll=4)

    def build_unpack():
        edges = lax.broadcasted_iota(jnp.int32, (EP, 1), 0) * tok_rows
        row = chosen[pl.ds(block, 1), :]
        lo, hi = count(row < edges), count(row < edges + tok_rows)
        lead = lo + ((lo + c) & 1)
        base = (lead - c) >> 1
        filled = (hi - lead + 1) >> 1
        ahead = lax.broadcasted_iota(jnp.int32, (1, rows), 1) - base
        rank[...] = jnp.where((ahead >= 0) & (ahead < filled), ahead, -1)

        def body(i, _):
            made = [
                jnp.where(rank[pl.ds(2 * i + k, 1), :] == slot_steps, 1.0, 0.0) for k in range(2)
            ]
            unpack[pl.ds(pl.multiple_of(i * pair, pair), pair), :] = jnp.concatenate(made, axis=0).astype(BF)
            return 0

        lax.fori_loop(0, EP // 2, body, 0, unroll=4)
        unpack_t[...] = unpack[...].T

    def build_factor():
        step = min(LANES, rows)

        def body(i, _):
            at = pl.ds(pl.multiple_of(i * step, step), step)
            wanted = 2 * (lax.broadcasted_iota(jnp.int32, (step, 1), 0) + i * step) + c
            found = jnp.where(positions == wanted, rw[...], 0.0)
            factor[at, :] = jnp.broadcast_to(jnp.sum(found, axis=1, keepdims=True), (step, LANES))
            return 0

        lax.fori_loop(0, rows // step, body, 0)

    build_place(0)
    tok_copy.wait()
    for copy in small[1:]:
        copy.wait()
    squares = jnp.zeros((tok_v.shape[0], 1), F32)
    for part_at in range(0, model, 512):
        some = tok_v[:, pl.ds(part_at, 512)].astype(F32)
        squares = squares + jnp.sum(some * some, axis=-1, keepdims=True)
    scale = lax.rsqrt(squares / model + 1e-06)
    def normed(start, size):
        columns = pl.ds(pl.multiple_of(start, LANES), size)
        return (tok_v[:, columns].astype(F32) * scale * gain[:, columns]).astype(BF)

    def pack(some, q):
        packed = jnp.dot(place[pl.ds(0, half_slots), :], some, preferred_element_type=F32)
        for h in range(some.shape[1] // LANES):
            sendbuf[q + h] = packed[:, h * LANES:(h + 1) * LANES].astype(BF).reshape(EP, slots, LANES)

    def exchange(q):
        def body(i, _):
            other = peer(i)
            remote(
                sendbuf.at[q, other], recvbuf.at[q, block], ep_send.at[q], ep_recv.at[q], chip(other, c)
            ).start()
            return 0

        lax.fori_loop(1, EP, body, 0)
        COPY(sendbuf.at[q, block], recvbuf.at[q, block], ep_recv.at[q]).start()

    pack(normed(y * width, width), 0)
    pl.semaphore_wait(barrier, plane - 1 + 2)
    exchange(0)
    exchange(1)
    pack(normed(wrap(y + FAR) * width, width), 2)

    sibling = (z, x, y, 1 - c)
    shared = [
        remote(gate, gu_v.at[:, pl.ds(2 * ff, ff)], wx_send.at[0], wx_recv.at[0], sibling),
        remote(up, gu_v.at[:, pl.ds(3 * ff, ff)], wx_send.at[1], wx_recv.at[1], sibling),
        remote(down, dw_v.at[pl.ds(ff, ff), :], wx_send.at[2], wx_recv.at[2], sibling),
    ]
    for copy in shared:
        copy.start()
    for q in range(2, 4):
        exchange(q)
    build_unpack()

    def ag_copy(way, u, h):
        source = wrap(y + ((0, -1, FAR) if way == 0 else (0, 1, FAR))[u])
        where = ag.at[h, source]
        return remote(where, where, ag_send.at[way, u, h], ag_recv.at[way, u, h], along(way))

    def compact(q):
        COPY(recvbuf.at[q], recvbuf.at[q], ep_recv.at[q]).wait()
        u, h = q // 2, q % 2
        ag[h, wrap(y + u * FAR)] = jnp.dot(
            unpack_t[...], recvbuf[q].reshape(half_slots, LANES), preferred_element_type=F32
        ).astype(BF)
        for way in range(2):
            ag_copy(way, 2 * u, h).start()

    def gather_in(parts, begin=False):
        x_rows = jnp.concatenate([ag[h, source] for h, source in parts], axis=1)

        def tile(n, _):
            n_at = pl.ds(pl.multiple_of(n * ff, ff), ff)
            weight = jnp.concatenate(
                [gu_v[pl.ds(pl.multiple_of(source * width + h * LANES, LANES), LANES), n_at] for h, source in parts],
                axis=0,
            )
            product = jnp.dot(x_rows, weight, preferred_element_type=F32)
            if begin:
                acc[:, n_at] = product
            else:
                acc[:, n_at] += product
            return 0

        lax.fori_loop(0, 4, tile, 0)

    def whole(offset):
        source = wrap(y + offset)
        return [(0, source), (1, source)]

    compact(0)
    build_factor()
    build_place(1)
    place_t[...] = place[...].T
    compact(1)
    for copy in own:
        copy.wait()
    for copy in shared[:2]:
        copy.wait_recv()
    gather_in(whole(0), True)
    for h in range(2):
        for way in range(2):
            ag_copy(way, 0, h).wait_recv()
            ag_copy(way, 1, h).start()
    for offset in (-1, 1):
        gather_in(whole(offset))
    for q in (2, 3):
        compact(q)
    gather_in(whole(FAR))
    for way in range(2):
        for h in range(2):
            ag_copy(way, 1, h).wait_recv()
        gather_in(whole((-2, 2)[way]))
    for h in range(2):
        for way in range(2):
            ag_copy(way, 2, h).wait_recv()
        gather_in([(h, wrap(y - 1 + FAR)), (h, wrap(y + 1 + FAR))])

    for s in range(2):
        gate_pre = acc[:, pl.ds(2 * s * ff, ff)]
        up_pre = acc[:, pl.ds((2 * s + 1) * ff, ff)]
        hidden[:, pl.ds(s * ff, ff)] = (gate_pre / (1.0 + jnp.exp(-gate_pre)) * up_pre).astype(BF)
    shared[2].wait_recv()

    def terms(offset):
        target = wrap(y + offset)
        part[offset % NY] = jnp.dot(
            hidden[...], dw_v[:, pl.ds(pl.multiple_of(target * width, width), width)],
            preferred_element_type=F32,
        )

    piece = [pl.ds(0, rows // 2), pl.ds(rows // 2, rows // 2)]

    def rs_copy(way, h, hop, s):
        source = rs_first.at[way, h] if hop == 0 else rs.at[way, h, hop - 1, piece[s]]
        return remote(
            source, rs.at[way, h, hop, piece[s]],
            rs_send.at[way, h, hop, s], rs_recv.at[way, h, hop, s], along(way),
        )

    def pass_on(way, h, hop, s):
        ahead = FAR - hop if way == 0 else hop - FAR
        mine = part[ahead % NY, piece[s], pl.ds(h * LANES, LANES)]
        if hop == 0:
            rs_first[way, h] = mine.astype(BF)
        else:
            if hop > 1 or s == way:
                rs_copy(way, h, hop - 1, s).wait_recv()
                mine = mine + rs[way, h, hop - 1, piece[s]].astype(F32)
            rs[way, h, hop - 1, piece[s]] = mine.astype(BF)
        rs_copy(way, h, hop, s).start()

    def each_way(h, hop, chained):
        for way in range(2):
            pass_on(way, h, hop, way if chained else 1 - way)

    def finish(h):
        for way in range(2):
            for s in range(2):
                rs_copy(way, h, FAR - 1, s).wait_recv()
        total = part[0, :, pl.ds(h * LANES, LANES)]
        for way in range(2):
            total = total + rs[way, h, FAR - 1].astype(F32)
        weighted = (total * factor[...]).astype(BF)
        back[h] = (
            jnp.dot(unpack[...], weighted, preferred_element_type=F32).astype(BF).reshape(EP, slots, LANES)
        )
        rel = lax.rem(c + h, 2)

        def give(i, _):
            other = peer(i)
            remote(back.at[h, other], ret.at[rel, block], ret_send, ret_recv, chip(other, h)).start()
            return 0

        lax.fori_loop(1, EP, give, 0)

        @pl.when(c == h)
        def _():
            COPY(back.at[h, block], ret.at[rel, block], ret_recv).start()

        @pl.when(c != h)
        def _():
            remote(back.at[h, block], ret.at[rel, block], ret_send, ret_recv, chip(block, h)).start()

    terms(FAR)
    for h in range(2):
        each_way(h, 0, True)
    for offset in (FAR - 1, 1 - FAR):
        terms(offset)
    for h in range(2):
        each_way(h, 1, False)
    for hop in range(2, FAR):
        for offset in (FAR - hop, hop - FAR):
            terms(offset)
    terms(0)
    for h in range(2):
        each_way(h, 1, True)
    for hop in range(2, FAR):
        for h in range(2):
            for chained in (False, True):
                each_way(h, hop, chained)
    for h in range(2):
        finish(h)

    for q in range(4):
        sent = sendbuf.at[q, pl.ds(0, EP - 1)]
        COPY(sent, sent, ep_send.at[q]).wait()
    for h in range(2):
        for way in range(2):
            for u in range(3):
                ag_copy(way, u, h).wait_send()
            for hop in range(FAR):
                for s in range(2):
                    if hop > 0 or s == way:
                        rs_copy(way, h, hop, s).wait_send()
    for copy in shared:
        copy.wait_send()
    COPY(ret, ret, ret_recv).wait()
    out[...] = jnp.dot(
        place_t[...], ret[...].reshape(2 * half_slots, LANES), preferred_element_type=F32
    ).astype(BF)
    for h in range(2):
        sent = back.at[h, pl.ds(0, EP - h)]
        COPY(sent, sent, ret_send).wait()


def shards(tokens, norm_gain, chosen, route_weight, gate_weight, up_weight, down_weight):
    tok_rows, model = tokens.shape
    experts, capacity = chosen.shape
    ff = gate_weight.shape[2]
    slots = 3 * tok_rows // 32
    rows = capacity // 2
    vmem = pl.BlockSpec(memory_space=pltpu.VMEM)
    hbm = pl.BlockSpec(memory_space=pl.ANY)
    dma = pltpu.SemaphoreType.DMA
    return pl.pallas_call(
        functools.partial(kernel, slots),
        out_shape=pltpu.VMEM((tok_rows, model // (NY * NC)), BF),
        in_specs=[hbm] * 7,
        out_specs=vmem,
        scratch_shapes=[
            pltpu.VMEM((tok_rows, model), BF),
            pltpu.VMEM((1, model), F32),
            pltpu.VMEM((experts, capacity), jnp.int32),
            pltpu.VMEM((1, capacity), F32),
            pltpu.VMEM((model, 4 * ff), BF),
            pltpu.VMEM((2 * ff, model), BF),
            pltpu.VMEM((experts, capacity), F32),
            pltpu.VMEM((experts, capacity), jnp.int32),
            pltpu.VMEM((EP, rows), jnp.int32),
            pltpu.VMEM((rows, LANES), F32),
            pltpu.VMEM((2 * EP * slots, tok_rows), BF),
            pltpu.VMEM((tok_rows, 2 * EP * slots), BF),
            pltpu.VMEM((EP * slots, rows), BF),
            pltpu.VMEM((rows, EP * slots), BF),
            pltpu.VMEM((4, EP, slots, LANES), BF),
            pltpu.VMEM((4, EP, slots, LANES), BF),
            pltpu.VMEM((2, NY, rows, LANES), BF),
            pltpu.VMEM((rows, 4 * ff), F32),
            pltpu.VMEM((rows, 2 * ff), BF),
            pltpu.VMEM((NY, rows, 2 * LANES), F32),
            pltpu.VMEM((2, 2, rows // 2, LANES), BF),
            pltpu.VMEM((2, 2, FAR, rows, LANES), BF),
            pltpu.VMEM((2, EP, slots, LANES), BF),
            pltpu.VMEM((2, EP, slots, LANES), BF),
            dma(()),
            dma((3,)),
            dma((3,)),
            dma((3,)),
            dma((3,)),
            dma((4,)),
            dma((4,)),
            dma((2, 3, 2)),
            dma((2, 3, 2)),
            dma((2, 2, FAR, 2)),
            dma((2, 2, FAR, 2)),
            dma(()),
            dma(()),
        ],
        compiler_params=pltpu.CompilerParams(
            collective_id=0, has_side_effects=True, vmem_limit_bytes=56 * 1024 * 1024
        ),
    )(tokens, norm_gain.reshape(1, -1), chosen, route_weight, gate_weight[0], up_weight[0], down_weight[0])


def solution(mesh):
    finer = Mesh(mesh.devices.reshape(NZ, NX, NY, NC), ("z", "x", "y", "c"))
    ep, tp = ("z", "x"), ("y", "c")
    in_specs = (
        P(ep, None),
        P(),
        P(),
        P(ep, None),
        P(ep, None, tp),
        P(ep, None, tp),
        P(ep, tp, None),
    )
    return jax.shard_map(
        shards, mesh=finer, in_specs=in_specs, out_specs=P(ep, tp), check_vma=False
    )
```

```python
import functools

import jax
import jax.numpy as jnp
from jax import lax
from jax.experimental import pallas as pl
from jax.experimental.pallas import tpu as pltpu
from jax.sharding import Mesh
from jax.sharding import PartitionSpec as P

NZ, NX, NY, NC = 8, 4, 8, 2
EP = NZ * NX
BF = jnp.bfloat16
F32 = jnp.float32
LANES = 128
COPY = pltpu.make_async_copy


def remote(src, dst, send, recv, where):
    return pltpu.make_async_remote_copy(
        src_ref=src, dst_ref=dst, send_sem=send, recv_sem=recv,
        device_id=where, device_id_type=pl.DeviceIdType.MESH,
    )


FAR = NY // 2


def kernel(
    slots, tokens, gain_in, chosen_in, rw_in, gate, up, down, out,
    tok_v, gain, chosen, rw, gu_v, dw_v, values, dist, rank, factor, place, place_t, unpack, unpack_t, sendbuf, recvbuf, ag, acc, hidden, part, rs_first, rs, back, ret,
    tok_sem, in_sem, w_sem, wx_send, wx_recv, ep_send, ep_recv, ag_send, ag_recv, rs_send, rs_recv, ret_send, ret_recv,
):
    z, x = lax.axis_index("z"), lax.axis_index("x")
    y, c = lax.axis_index("y"), lax.axis_index("c")
    block = z * NX + x
    rows = ag.shape[2]
    width = 2 * LANES
    ff = gate.shape[1]
    model = tokens.shape[1]
    half_slots = EP * slots

    def wrap(v):
        return lax.rem(v + NY, NY)

    def chip(index, core):
        return (index // NX, lax.rem(index, NX), y, core)

    def along(way):
        return (z, x, wrap(y + 1) if way == 0 else wrap(y - 1), c)

    small = [
        COPY(chosen_in, chosen, in_sem.at[0]),
        COPY(gain_in, gain, in_sem.at[1]),
        COPY(rw_in, rw, in_sem.at[2]),
    ]
    small[0].start()
    tok_copy = COPY(tokens, tok_v, tok_sem)
    tok_copy.start()
    for copy in small[1:]:
        copy.start()
    own = [
        COPY(gate, gu_v.at[:, pl.ds(0, ff)], w_sem.at[0]),
        COPY(up, gu_v.at[:, pl.ds(ff, ff)], w_sem.at[1]),
        COPY(down, dw_v.at[pl.ds(0, ff), :], w_sem.at[2]),
    ]
    for copy in own:
        copy.start()

    def peer(i):
        step = (i + 1) // 2
        return lax.rem(block + jnp.where(lax.rem(i, 2) == 1, step, EP - step), EP)

    barrier = pltpu.get_barrier_semaphore()
    plane = EP * NC
    apart = sorted(range(NZ), key=lambda dz: -min(dz, NZ - dz))
    for dz in apart:
        for dx in range(NX - 1, -1, -1):
            for dc in range(NC):
                if dz or dx or dc:
                    pl.semaphore_signal(
                        barrier, inc=1,
                        device_id=(lax.rem(z + dz, NZ), lax.rem(x + dx, NX), y, lax.rem(c + dc, NC)),
                        device_id_type=pl.DeviceIdType.MESH,
                    )
    for way in range(2):
        pl.semaphore_signal(barrier, inc=1, device_id=along(way), device_id_type=pl.DeviceIdType.MESH)

    tok_rows, capacity = tok_v.shape[0], chosen.shape[1]
    first = block * tok_rows
    pair = 2 * slots
    slot_steps = lax.broadcasted_iota(jnp.int32, (slots, 1), 0)
    positions = lax.broadcasted_iota(jnp.int32, (1, capacity), 1)

    def count(hits):
        return jnp.sum(jnp.where(hits, 1.0, 0.0), axis=1, keepdims=True).astype(jnp.int32)

    small[0].wait()
    run_start = count(chosen[...] < first)
    values[...] = (chosen[...] - (first - 1)).astype(F32)
    token_ids = (lax.broadcasted_iota(jnp.int32, (1, tok_rows), 1) + 1).astype(F32)

    def build_place(rel):
        parity = lax.rem(c + rel, 2)
        lead = run_start + ((run_start + parity) & 1)
        dist[...] = positions - lead

        def body(i, _):
            made = []
            for k in range(2):
                at = pl.ds(2 * i + k, 1)
                found = jnp.where(dist[at, :] == 2 * slot_steps, values[at, :], 0.0)
                token = jnp.sum(found, axis=1, keepdims=True)
                made.append(jnp.where(token == token_ids, 1.0, 0.0))
            to = pl.ds(pl.multiple_of(rel * half_slots + i * pair, pair), pair)
            place[to, :] = jnp.concatenate(made, axis=0).astype(BF)
            return 0

        lax.fori_loop(0, EP // 2, body, 0, unroll=4)

    def build_unpack():
        edges = lax.broadcasted_iota(jnp.int32, (EP, 1), 0) * tok_rows
        row = chosen[pl.ds(block, 1), :]
        lo, hi = count(row < edges), count(row < edges + tok_rows)
        lead = lo + ((lo + c) & 1)
        base = (lead - c) >> 1
        filled = (hi - lead + 1) >> 1
        ahead = lax.broadcasted_iota(jnp.int32, (1, rows), 1) - base
        rank[...] = jnp.where((ahead >= 0) & (ahead < filled), ahead, -1)

        def body(i, _):
            made = [
                jnp.where(rank[pl.ds(2 * i + k, 1), :] == slot_steps, 1.0, 0.0) for k in range(2)
            ]
            unpack[pl.ds(pl.multiple_of(i * pair, pair), pair), :] = jnp.concatenate(made, axis=0).astype(BF)
            return 0

        lax.fori_loop(0, EP // 2, body, 0, unroll=4)
        unpack_t[...] = unpack[...].T

    def build_factor():
        step = min(LANES, rows)

        def body(i, _):
            at = pl.ds(pl.multiple_of(i * step, step), step)
            wanted = 2 * (lax.broadcasted_iota(jnp.int32, (step, 1), 0) + i * step) + c
            found = jnp.where(positions == wanted, rw[...], 0.0)
            factor[at, :] = jnp.broadcast_to(jnp.sum(found, axis=1, keepdims=True), (step, LANES))
            return 0

        lax.fori_loop(0, rows // step, body, 0)

    build_place(0)
    tok_copy.wait()
    for copy in small[1:]:
        copy.wait()
    squares = jnp.zeros((tok_v.shape[0], 1), F32)
    for part_at in range(0, model, 512):
        some = tok_v[:, pl.ds(part_at, 512)].astype(F32)
        squares = squares + jnp.sum(some * some, axis=-1, keepdims=True)
    scale = lax.rsqrt(squares / model + 1e-06)
    def normed(start, size):
        columns = pl.ds(pl.multiple_of(start, LANES), size)
        return (tok_v[:, columns].astype(F32) * scale * gain[:, columns]).astype(BF)

    def pack(some, q):
        packed = jnp.dot(place[pl.ds(0, half_slots), :], some, preferred_element_type=F32)
        for h in range(some.shape[1] // LANES):
            sendbuf[q + h] = packed[:, h * LANES:(h + 1) * LANES].astype(BF).reshape(EP, slots, LANES)

    def exchange(q):
        def body(i, _):
            other = peer(i)
            remote(
                sendbuf.at[q, other], recvbuf.at[q, block], ep_send.at[q], ep_recv.at[q], chip(other, c)
            ).start()
            return 0

        lax.fori_loop(1, EP, body, 0)
        COPY(sendbuf.at[q, block], recvbuf.at[q, block], ep_recv.at[q]).start()

    pack(normed(y * width, width), 0)
    pl.semaphore_wait(barrier, plane - 1 + 2)
    exchange(0)
    exchange(1)
    pack(normed(wrap(y + FAR) * width, width), 2)

    sibling = (z, x, y, 1 - c)
    shared = [
        remote(gate, gu_v.at[:, pl.ds(2 * ff, ff)], wx_send.at[0], wx_recv.at[0], sibling),
        remote(up, gu_v.at[:, pl.ds(3 * ff, ff)], wx_send.at[1], wx_recv.at[1], sibling),
        remote(down, dw_v.at[pl.ds(ff, ff), :], wx_send.at[2], wx_recv.at[2], sibling),
    ]
    for copy in shared:
        copy.start()
    for q in range(2, 4):
        exchange(q)
    build_unpack()

    piece = [pl.ds(0, rows // 2), pl.ds(rows // 2, rows // 2)]

    def ag_copy(way, u, h, s=None):
        source = wrap(y + ((0, -1, FAR) if way == 0 else (0, 1, FAR))[u])
        where = ag.at[h, source] if s is None else ag.at[h, source, piece[s]]
        at = (way, u, h, 0 if s is None else s)
        return remote(where, where, ag_send.at[at], ag_recv.at[at], along(way))

    def send_on(u, h, s=None):
        for way in range(2):
            ag_copy(way, u, h, s).start()

    def compact(q):
        COPY(recvbuf.at[q], recvbuf.at[q], ep_recv.at[q]).wait()
        u, h = q // 2, q % 2
        ag[h, wrap(y + u * FAR)] = jnp.dot(
            unpack_t[...], recvbuf[q].reshape(half_slots, LANES), preferred_element_type=F32
        ).astype(BF)

    def gather_in(parts, begin=False, r_at=pl.ds(0, rows)):
        x_rows = jnp.concatenate([ag[h, source, r_at] for h, source in parts], axis=1)

        def tile(n, _):
            n_at = pl.ds(pl.multiple_of(n * ff, ff), ff)
            weight = jnp.concatenate(
                [gu_v[pl.ds(pl.multiple_of(source * width + h * LANES, LANES), LANES), n_at] for h, source in parts],
                axis=0,
            )
            product = jnp.dot(x_rows, weight, preferred_element_type=F32)
            if begin:
                acc[r_at, n_at] = product
            else:
                acc[r_at, n_at] += product
            return 0

        lax.fori_loop(0, 4, tile, 0)

    def whole(offset):
        source = wrap(y + offset)
        return [(0, source), (1, source)]

    compact(0)
    send_on(0, 0)
    build_factor()
    build_place(1)
    place_t[...] = place[...].T
    compact(1)
    send_on(0, 1)
    for copy in own:
        copy.wait()
    for copy in shared[:2]:
        copy.wait_recv()
    gather_in(whole(0), True)
    for h in range(2):
        for way in range(2):
            ag_copy(way, 0, h).wait_recv()
            ag_copy(way, 1, h).start()
    for offset in (-1, 1):
        gather_in(whole(offset))
    compact(2)
    send_on(2, 0, 0)
    compact(3)
    for h, s in ((1, 0), (0, 1), (1, 1)):
        send_on(2, h, s)
    gather_in(whole(FAR))
    for way in range(2):
        for h in range(2):
            ag_copy(way, 1, h).wait_recv()
        gather_in(whole((-2, 2)[way]))

    def rest(s):
        for h in range(2):
            for way in range(2):
                ag_copy(way, 2, h, s).wait_recv()
            gather_in([(h, wrap(y - 1 + FAR)), (h, wrap(y + 1 + FAR))], r_at=piece[s])
        for n in range(2):
            gate_pre = acc[piece[s], pl.ds(2 * n * ff, ff)]
            up_pre = acc[piece[s], pl.ds((2 * n + 1) * ff, ff)]
            hidden[piece[s], pl.ds(n * ff, ff)] = (gate_pre / (1.0 + jnp.exp(-gate_pre)) * up_pre).astype(BF)

    def terms(offset, s):
        target = wrap(y + offset)
        part[offset % NY, piece[s]] = jnp.dot(
            hidden[piece[s], :], dw_v[:, pl.ds(pl.multiple_of(target * width, width), width)],
            preferred_element_type=F32,
        )

    def rs_copy(way, h, hop, s):
        source = rs_first.at[way, h] if hop == 0 else rs.at[way, h, hop - 1, piece[s]]
        return remote(
            source, rs.at[way, h, hop, piece[s]],
            rs_send.at[way, h, hop, s], rs_recv.at[way, h, hop, s], along(way),
        )

    def pass_on(way, h, hop, s):
        ahead = FAR - hop if way == 0 else hop - FAR
        mine = part[ahead % NY, piece[s], pl.ds(h * LANES, LANES)]
        if hop == 0:
            rs_first[way, h] = mine.astype(BF)
        else:
            if hop > 1 or s == way:
                rs_copy(way, h, hop - 1, s).wait_recv()
                mine = mine + rs[way, h, hop - 1, piece[s]].astype(F32)
            rs[way, h, hop - 1, piece[s]] = mine.astype(BF)
        rs_copy(way, h, hop, s).start()

    def each_way(h, hop, chained):
        for way in range(2):
            pass_on(way, h, hop, way if chained else 1 - way)

    def finish(h):
        for way in range(2):
            for s in range(2):
                rs_copy(way, h, FAR - 1, s).wait_recv()
        total = part[0, :, pl.ds(h * LANES, LANES)]
        for way in range(2):
            total = total + rs[way, h, FAR - 1].astype(F32)
        weighted = (total * factor[...]).astype(BF)
        back[h] = (
            jnp.dot(unpack[...], weighted, preferred_element_type=F32).astype(BF).reshape(EP, slots, LANES)
        )
        rel = lax.rem(c + h, 2)

        def give(i, _):
            other = peer(i)
            remote(back.at[h, other], ret.at[rel, block], ret_send, ret_recv, chip(other, h)).start()
            return 0

        lax.fori_loop(1, EP, give, 0)

        @pl.when(c == h)
        def _():
            COPY(back.at[h, block], ret.at[rel, block], ret_recv).start()

        @pl.when(c != h)
        def _():
            remote(back.at[h, block], ret.at[rel, block], ret_send, ret_recv, chip(block, h)).start()

    for s in range(2):
        rest(s)
        if s == 0:
            shared[2].wait_recv()
        terms(FAR, s)
        for h in range(2):
            pass_on(s, h, 0, s)
        near = 1 - FAR if s == 0 else FAR - 1
        terms(near, s)
        for h in range(2):
            pass_on(1 - s, h, 1, s)
    terms(FAR - 1, 0)
    terms(1 - FAR, 1)
    for s in range(2):
        for hop in range(2, FAR):
            for offset in (FAR - hop, hop - FAR):
                terms(offset, s)
    for h in range(2):
        each_way(h, 1, True)
    for s in range(2):
        terms(0, s)
    for hop in range(2, FAR):
        for h in range(2):
            for chained in (False, True):
                each_way(h, hop, chained)
    for h in range(2):
        finish(h)

    for q in range(4):
        sent = sendbuf.at[q, pl.ds(0, EP - 1)]
        COPY(sent, sent, ep_send.at[q]).wait()
    for h in range(2):
        for way in range(2):
            for u in range(2):
                ag_copy(way, u, h).wait_send()
            for s in range(2):
                ag_copy(way, 2, h, s).wait_send()
            for hop in range(FAR):
                for s in range(2):
                    if hop > 0 or s == way:
                        rs_copy(way, h, hop, s).wait_send()
    for copy in shared:
        copy.wait_send()
    COPY(ret, ret, ret_recv).wait()
    out[...] = jnp.dot(
        place_t[...], ret[...].reshape(2 * half_slots, LANES), preferred_element_type=F32
    ).astype(BF)
    for h in range(2):
        sent = back.at[h, pl.ds(0, EP - h)]
        COPY(sent, sent, ret_send).wait()


def shards(tokens, norm_gain, chosen, route_weight, gate_weight, up_weight, down_weight):
    tok_rows, model = tokens.shape
    experts, capacity = chosen.shape
    ff = gate_weight.shape[2]
    slots = 3 * tok_rows // 32
    rows = capacity // 2
    vmem = pl.BlockSpec(memory_space=pltpu.VMEM)
    hbm = pl.BlockSpec(memory_space=pl.ANY)
    dma = pltpu.SemaphoreType.DMA
    return pl.pallas_call(
        functools.partial(kernel, slots),
        out_shape=pltpu.VMEM((tok_rows, model // (NY * NC)), BF),
        in_specs=[hbm] * 7,
        out_specs=vmem,
        scratch_shapes=[
            pltpu.VMEM((tok_rows, model), BF),
            pltpu.VMEM((1, model), F32),
            pltpu.VMEM((experts, capacity), jnp.int32),
            pltpu.VMEM((1, capacity), F32),
            pltpu.VMEM((model, 4 * ff), BF),
            pltpu.VMEM((2 * ff, model), BF),
            pltpu.VMEM((experts, capacity), F32),
            pltpu.VMEM((experts, capacity), jnp.int32),
            pltpu.VMEM((EP, rows), jnp.int32),
            pltpu.VMEM((rows, LANES), F32),
            pltpu.VMEM((2 * EP * slots, tok_rows), BF),
            pltpu.VMEM((tok_rows, 2 * EP * slots), BF),
            pltpu.VMEM((EP * slots, rows), BF),
            pltpu.VMEM((rows, EP * slots), BF),
            pltpu.VMEM((4, EP, slots, LANES), BF),
            pltpu.VMEM((4, EP, slots, LANES), BF),
            pltpu.VMEM((2, NY, rows, LANES), BF),
            pltpu.VMEM((rows, 4 * ff), F32),
            pltpu.VMEM((rows, 2 * ff), BF),
            pltpu.VMEM((NY, rows, 2 * LANES), F32),
            pltpu.VMEM((2, 2, rows // 2, LANES), BF),
            pltpu.VMEM((2, 2, FAR, rows, LANES), BF),
            pltpu.VMEM((2, EP, slots, LANES), BF),
            pltpu.VMEM((2, EP, slots, LANES), BF),
            dma(()),
            dma((3,)),
            dma((3,)),
            dma((3,)),
            dma((3,)),
            dma((4,)),
            dma((4,)),
            dma((2, 3, 2, 2)),
            dma((2, 3, 2, 2)),
            dma((2, 2, FAR, 2)),
            dma((2, 2, FAR, 2)),
            dma(()),
            dma(()),
        ],
        compiler_params=pltpu.CompilerParams(
            collective_id=0, has_side_effects=True, vmem_limit_bytes=56 * 1024 * 1024
        ),
    )(tokens, norm_gain.reshape(1, -1), chosen, route_weight, gate_weight[0], up_weight[0], down_weight[0])


def solution(mesh):
    finer = Mesh(mesh.devices.reshape(NZ, NX, NY, NC), ("z", "x", "y", "c"))
    ep, tp = ("z", "x"), ("y", "c")
    in_specs = (
        P(ep, None),
        P(),
        P(),
        P(ep, None),
        P(ep, None, tp),
        P(ep, None, tp),
        P(ep, tp, None),
    )
    return jax.shard_map(
        shards, mesh=finer, in_specs=in_specs, out_specs=P(ep, tp), check_vma=False
    )
```

```python
import functools

import jax
import jax.numpy as jnp
from jax import lax
from jax.experimental import pallas as pl
from jax.experimental.pallas import tpu as pltpu
from jax.sharding import Mesh
from jax.sharding import PartitionSpec as P

NZ, NX, NY, NC = 8, 4, 8, 2
EP = NZ * NX
BF = jnp.bfloat16
F32 = jnp.float32
LANES = 128
COPY = pltpu.make_async_copy


def remote(src, dst, send, recv, where):
    return pltpu.make_async_remote_copy(
        src_ref=src, dst_ref=dst, send_sem=send, recv_sem=recv,
        device_id=where, device_id_type=pl.DeviceIdType.MESH,
    )


FAR = NY // 2


def kernel(
    slots, tokens, gain_in, chosen_in, rw_in, gate, up, down, out,
    tok_v, gain, chosen, rw, gu_v, dw_v, values, dist, rank, factor, place, place_t, unpack, unpack_t, sendbuf, recvbuf, ag, acc, hidden, part, rs_first, rs, back, ret,
    tok_sem, in_sem, w_sem, wx_send, wx_recv, ep_send, ep_recv, ag_send, ag_recv, rs_send, rs_recv, ret_send, ret_recv,
):
    z, x = lax.axis_index("z"), lax.axis_index("x")
    y, c = lax.axis_index("y"), lax.axis_index("c")
    block = z * NX + x
    rows = ag.shape[2]
    width = 2 * LANES
    ff = gate.shape[1]
    model = tokens.shape[1]
    half_slots = EP * slots

    def wrap(v):
        return lax.rem(v + NY, NY)

    def chip(index, core):
        return (index // NX, lax.rem(index, NX), y, core)

    def along(way):
        return (z, x, wrap(y + 1) if way == 0 else wrap(y - 1), c)

    small = [
        COPY(chosen_in, chosen, in_sem.at[0]),
        COPY(gain_in, gain, in_sem.at[1]),
        COPY(rw_in, rw, in_sem.at[2]),
    ]
    small[0].start()
    tok_copy = COPY(tokens, tok_v, tok_sem)
    tok_copy.start()
    for copy in small[1:]:
        copy.start()
    own = [
        COPY(gate, gu_v.at[:, pl.ds(0, ff)], w_sem.at[0]),
        COPY(up, gu_v.at[:, pl.ds(ff, ff)], w_sem.at[1]),
        COPY(down, dw_v.at[pl.ds(0, ff), :], w_sem.at[2]),
    ]
    for copy in own:
        copy.start()

    def peer(i):
        step = (i + 1) // 2
        return lax.rem(block + jnp.where(lax.rem(i, 2) == 1, step, EP - step), EP)

    barrier = pltpu.get_barrier_semaphore()
    plane = EP * NC
    apart = sorted(range(NZ), key=lambda dz: -min(dz, NZ - dz))
    for dz in apart:
        for dx in range(NX - 1, -1, -1):
            for dc in range(NC):
                if dz or dx or dc:
                    pl.semaphore_signal(
                        barrier, inc=1,
                        device_id=(lax.rem(z + dz, NZ), lax.rem(x + dx, NX), y, lax.rem(c + dc, NC)),
                        device_id_type=pl.DeviceIdType.MESH,
                    )
    for way in range(2):
        pl.semaphore_signal(barrier, inc=1, device_id=along(way), device_id_type=pl.DeviceIdType.MESH)

    tok_rows, capacity = tok_v.shape[0], chosen.shape[1]
    first = block * tok_rows
    pair = 2 * slots
    slot_steps = lax.broadcasted_iota(jnp.int32, (slots, 1), 0)
    positions = lax.broadcasted_iota(jnp.int32, (1, capacity), 1)

    def count(hits):
        return jnp.sum(jnp.where(hits, 1.0, 0.0), axis=1, keepdims=True).astype(jnp.int32)

    small[0].wait()
    run_start = count(chosen[...] < first)
    values[...] = (chosen[...] - (first - 1)).astype(F32)
    token_ids = (lax.broadcasted_iota(jnp.int32, (1, tok_rows), 1) + 1).astype(F32)

    def build_place(rel):
        parity = lax.rem(c + rel, 2)
        lead = run_start + ((run_start + parity) & 1)
        dist[...] = positions - lead

        def body(i, _):
            made = []
            for k in range(2):
                at = pl.ds(2 * i + k, 1)
                found = jnp.where(dist[at, :] == 2 * slot_steps, values[at, :], 0.0)
                token = jnp.sum(found, axis=1, keepdims=True)
                made.append(jnp.where(token == token_ids, 1.0, 0.0))
            to = pl.ds(pl.multiple_of(rel * half_slots + i * pair, pair), pair)
            place[to, :] = jnp.concatenate(made, axis=0).astype(BF)
            return 0

        lax.fori_loop(0, EP // 2, body, 0, unroll=4)

    def build_unpack():
        edges = lax.broadcasted_iota(jnp.int32, (EP, 1), 0) * tok_rows
        row = chosen[pl.ds(block, 1), :]
        lo, hi = count(row < edges), count(row < edges + tok_rows)
        lead = lo + ((lo + c) & 1)
        base = (lead - c) >> 1
        filled = (hi - lead + 1) >> 1
        ahead = lax.broadcasted_iota(jnp.int32, (1, rows), 1) - base
        rank[...] = jnp.where((ahead >= 0) & (ahead < filled), ahead, -1)

        def body(i, _):
            made = [
                jnp.where(rank[pl.ds(2 * i + k, 1), :] == slot_steps, 1.0, 0.0) for k in range(2)
            ]
            unpack[pl.ds(pl.multiple_of(i * pair, pair), pair), :] = jnp.concatenate(made, axis=0).astype(BF)
            return 0

        lax.fori_loop(0, EP // 2, body, 0, unroll=4)
        unpack_t[...] = unpack[...].T

    def build_factor():
        step = min(LANES, rows)

        def body(i, _):
            at = pl.ds(pl.multiple_of(i * step, step), step)
            wanted = 2 * (lax.broadcasted_iota(jnp.int32, (step, 1), 0) + i * step) + c
            found = jnp.where(positions == wanted, rw[...], 0.0)
            factor[at, :] = jnp.broadcast_to(jnp.sum(found, axis=1, keepdims=True), (step, LANES))
            return 0

        lax.fori_loop(0, rows // step, body, 0)

    build_place(0)
    tok_copy.wait()
    for copy in small[1:]:
        copy.wait()
    squares = jnp.zeros((tok_v.shape[0], 1), F32)
    for part_at in range(0, model, 512):
        some = tok_v[:, pl.ds(part_at, 512)].astype(F32)
        squares = squares + jnp.sum(some * some, axis=-1, keepdims=True)
    scale = lax.rsqrt(squares / model + 1e-06)
    def normed(start, size):
        columns = pl.ds(pl.multiple_of(start, LANES), size)
        return (tok_v[:, columns].astype(F32) * scale * gain[:, columns]).astype(BF)

    def pack(some, q):
        packed = jnp.dot(place[pl.ds(0, half_slots), :], some, preferred_element_type=F32)
        for h in range(some.shape[1] // LANES):
            sendbuf[q + h] = packed[:, h * LANES:(h + 1) * LANES].astype(BF).reshape(EP, slots, LANES)

    def exchange(q):
        def body(i, _):
            other = peer(i)
            remote(
                sendbuf.at[q, other], recvbuf.at[q, block], ep_send.at[q], ep_recv.at[q], chip(other, c)
            ).start()
            return 0

        lax.fori_loop(1, EP, body, 0)
        COPY(sendbuf.at[q, block], recvbuf.at[q, block], ep_recv.at[q]).start()

    pack(normed(y * width, width), 0)
    pl.semaphore_wait(barrier, plane - 1 + 2)
    sibling = (z, x, y, 1 - c)
    shared = [
        remote(gate, gu_v.at[:, pl.ds(2 * ff, ff)], wx_send.at[0], wx_recv.at[0], sibling),
        remote(up, gu_v.at[:, pl.ds(3 * ff, ff)], wx_send.at[1], wx_recv.at[1], sibling),
        remote(down, dw_v.at[pl.ds(ff, ff), :], wx_send.at[2], wx_recv.at[2], sibling),
    ]
    for copy in shared:
        copy.start()
    exchange(0)
    exchange(1)
    pack(normed(wrap(y + FAR) * width, width), 2)

    for q in range(2, 4):
        exchange(q)
    build_unpack()

    piece = [pl.ds(0, rows // 2), pl.ds(rows // 2, rows // 2)]

    def ag_copy(way, u, h, s=None):
        source = wrap(y + ((0, -1, FAR) if way == 0 else (0, 1, FAR))[u])
        where = ag.at[h, source] if s is None else ag.at[h, source, piece[s]]
        at = (way, u, h, 0 if s is None else s)
        return remote(where, where, ag_send.at[at], ag_recv.at[at], along(way))

    def send_on(u, h, s=None):
        for way in range(2):
            ag_copy(way, u, h, s).start()

    def compact(q):
        COPY(recvbuf.at[q], recvbuf.at[q], ep_recv.at[q]).wait()
        u, h = q // 2, q % 2
        ag[h, wrap(y + u * FAR)] = jnp.dot(
            unpack_t[...], recvbuf[q].reshape(half_slots, LANES), preferred_element_type=F32
        ).astype(BF)

    def gather_in(parts, begin=False, r_at=pl.ds(0, rows)):
        x_rows = jnp.concatenate([ag[h, source, r_at] for h, source in parts], axis=1)

        def tile(n, _):
            n_at = pl.ds(pl.multiple_of(n * ff, ff), ff)
            weight = jnp.concatenate(
                [gu_v[pl.ds(pl.multiple_of(source * width + h * LANES, LANES), LANES), n_at] for h, source in parts],
                axis=0,
            )
            product = jnp.dot(x_rows, weight, preferred_element_type=F32)
            if begin:
                acc[r_at, n_at] = product
            else:
                acc[r_at, n_at] += product
            return 0

        lax.fori_loop(0, 4, tile, 0)

    def whole(offset):
        source = wrap(y + offset)
        return [(0, source), (1, source)]

    compact(0)
    send_on(0, 0)
    build_factor()
    build_place(1)
    place_t[...] = place[...].T
    compact(1)
    send_on(0, 1)
    for h in range(2):
        for way in range(2):
            ag_copy(way, 0, h).wait_recv()
            ag_copy(way, 1, h).start()
        if h == 0:
            for copy in own:
                copy.wait()
            for copy in shared[:2]:
                copy.wait_recv()
            gather_in(whole(0), True)
    for offset in (-1, 1):
        gather_in(whole(offset))
    compact(2)
    send_on(2, 0, 0)
    compact(3)
    for h, s in ((1, 0), (0, 1), (1, 1)):
        send_on(2, h, s)
    gather_in(whole(FAR))
    for way in range(2):
        for h in range(2):
            ag_copy(way, 1, h).wait_recv()
        gather_in(whole((-2, 2)[way]))

    def rest(s):
        for h in range(2):
            for way in range(2):
                ag_copy(way, 2, h, s).wait_recv()
            gather_in([(h, wrap(y - 1 + FAR)), (h, wrap(y + 1 + FAR))], r_at=piece[s])
        for n in range(2):
            gate_pre = acc[piece[s], pl.ds(2 * n * ff, ff)]
            up_pre = acc[piece[s], pl.ds((2 * n + 1) * ff, ff)]
            hidden[piece[s], pl.ds(n * ff, ff)] = (gate_pre / (1.0 + jnp.exp(-gate_pre)) * up_pre).astype(BF)

    def terms(offset, s):
        target = wrap(y + offset)
        part[offset % NY, piece[s]] = jnp.dot(
            hidden[piece[s], :], dw_v[:, pl.ds(pl.multiple_of(target * width, width), width)],
            preferred_element_type=F32,
        )

    def rs_copy(way, h, hop, s):
        source = rs_first.at[way, h] if hop == 0 else rs.at[way, h, hop - 1, piece[s]]
        return remote(
            source, rs.at[way, h, hop, piece[s]],
            rs_send.at[way, h, hop, s], rs_recv.at[way, h, hop, s], along(way),
        )

    def pass_on(way, h, hop, s):
        ahead = FAR - hop if way == 0 else hop - FAR
        mine = part[ahead % NY, piece[s], pl.ds(h * LANES, LANES)]
        if hop == 0:
            rs_first[way, h] = mine.astype(BF)
        else:
            if hop > 1 or s == way:
                rs_copy(way, h, hop - 1, s).wait_recv()
                mine = mine + rs[way, h, hop - 1, piece[s]].astype(F32)
            rs[way, h, hop - 1, piece[s]] = mine.astype(BF)
        rs_copy(way, h, hop, s).start()

    def each_way(h, hop, chained):
        for way in range(2):
            pass_on(way, h, hop, way if chained else 1 - way)

    def finish(h):
        for way in range(2):
            for s in range(2):
                rs_copy(way, h, FAR - 1, s).wait_recv()
        total = part[0, :, pl.ds(h * LANES, LANES)]
        for way in range(2):
            total = total + rs[way, h, FAR - 1].astype(F32)
        weighted = (total * factor[...]).astype(BF)
        back[h] = (
            jnp.dot(unpack[...], weighted, preferred_element_type=F32).astype(BF).reshape(EP, slots, LANES)
        )
        rel = lax.rem(c + h, 2)

        def give(i, _):
            other = peer(i)
            remote(back.at[h, other], ret.at[rel, block], ret_send, ret_recv, chip(other, h)).start()
            return 0

        lax.fori_loop(1, EP, give, 0)

        @pl.when(c == h)
        def _():
            COPY(back.at[h, block], ret.at[rel, block], ret_recv).start()

        @pl.when(c != h)
        def _():
            remote(back.at[h, block], ret.at[rel, block], ret_send, ret_recv, chip(block, h)).start()

    for s in range(2):
        rest(s)
        if s == 0:
            shared[2].wait_recv()
        terms(FAR, s)
        for h in range(2):
            pass_on(s, h, 0, s)
        near = 1 - FAR if s == 0 else FAR - 1
        terms(near, s)
        for h in range(2):
            pass_on(1 - s, h, 1, s)
    terms(FAR - 1, 0)
    terms(1 - FAR, 1)
    for s in range(2):
        for hop in range(2, FAR):
            for offset in (FAR - hop, hop - FAR):
                terms(offset, s)
    for h in range(2):
        each_way(h, 1, True)
    for s in range(2):
        terms(0, s)
    for hop in range(2, FAR):
        for h in range(2):
            for chained in (False, True):
                each_way(h, hop, chained)
    for h in range(2):
        finish(h)

    for q in range(4):
        sent = sendbuf.at[q, pl.ds(0, EP - 1)]
        COPY(sent, sent, ep_send.at[q]).wait()
    for h in range(2):
        for way in range(2):
            for u in range(2):
                ag_copy(way, u, h).wait_send()
            for s in range(2):
                ag_copy(way, 2, h, s).wait_send()
            for hop in range(FAR):
                for s in range(2):
                    if hop > 0 or s == way:
                        rs_copy(way, h, hop, s).wait_send()
    for copy in shared:
        copy.wait_send()
    COPY(ret, ret, ret_recv).wait()
    out[...] = jnp.dot(
        place_t[...], ret[...].reshape(2 * half_slots, LANES), preferred_element_type=F32
    ).astype(BF)
    for h in range(2):
        sent = back.at[h, pl.ds(0, EP - h)]
        COPY(sent, sent, ret_send).wait()


def shards(tokens, norm_gain, chosen, route_weight, gate_weight, up_weight, down_weight):
    tok_rows, model = tokens.shape
    experts, capacity = chosen.shape
    ff = gate_weight.shape[2]
    slots = 3 * tok_rows // 32
    rows = capacity // 2
    vmem = pl.BlockSpec(memory_space=pltpu.VMEM)
    hbm = pl.BlockSpec(memory_space=pl.ANY)
    dma = pltpu.SemaphoreType.DMA
    return pl.pallas_call(
        functools.partial(kernel, slots),
        out_shape=pltpu.VMEM((tok_rows, model // (NY * NC)), BF),
        in_specs=[hbm] * 7,
        out_specs=vmem,
        scratch_shapes=[
            pltpu.VMEM((tok_rows, model), BF),
            pltpu.VMEM((1, model), F32),
            pltpu.VMEM((experts, capacity), jnp.int32),
            pltpu.VMEM((1, capacity), F32),
            pltpu.VMEM((model, 4 * ff), BF),
            pltpu.VMEM((2 * ff, model), BF),
            pltpu.VMEM((experts, capacity), F32),
            pltpu.VMEM((experts, capacity), jnp.int32),
            pltpu.VMEM((EP, rows), jnp.int32),
            pltpu.VMEM((rows, LANES), F32),
            pltpu.VMEM((2 * EP * slots, tok_rows), BF),
            pltpu.VMEM((tok_rows, 2 * EP * slots), BF),
            pltpu.VMEM((EP * slots, rows), BF),
            pltpu.VMEM((rows, EP * slots), BF),
            pltpu.VMEM((4, EP, slots, LANES), BF),
            pltpu.VMEM((4, EP, slots, LANES), BF),
            pltpu.VMEM((2, NY, rows, LANES), BF),
            pltpu.VMEM((rows, 4 * ff), F32),
            pltpu.VMEM((rows, 2 * ff), BF),
            pltpu.VMEM((NY, rows, 2 * LANES), F32),
            pltpu.VMEM((2, 2, rows // 2, LANES), BF),
            pltpu.VMEM((2, 2, FAR, rows, LANES), BF),
            pltpu.VMEM((2, EP, slots, LANES), BF),
            pltpu.VMEM((2, EP, slots, LANES), BF),
            dma(()),
            dma((3,)),
            dma((3,)),
            dma((3,)),
            dma((3,)),
            dma((4,)),
            dma((4,)),
            dma((2, 3, 2, 2)),
            dma((2, 3, 2, 2)),
            dma((2, 2, FAR, 2)),
            dma((2, 2, FAR, 2)),
            dma(()),
            dma(()),
        ],
        compiler_params=pltpu.CompilerParams(
            collective_id=0, has_side_effects=True, vmem_limit_bytes=56 * 1024 * 1024
        ),
    )(tokens, norm_gain.reshape(1, -1), chosen, route_weight, gate_weight[0], up_weight[0], down_weight[0])


def solution(mesh):
    finer = Mesh(mesh.devices.reshape(NZ, NX, NY, NC), ("z", "x", "y", "c"))
    ep, tp = ("z", "x"), ("y", "c")
    in_specs = (
        P(ep, None),
        P(),
        P(),
        P(ep, None),
        P(ep, None, tp),
        P(ep, None, tp),
        P(ep, tp, None),
    )
    return jax.shard_map(
        shards, mesh=finer, in_specs=in_specs, out_specs=P(ep, tp), check_vma=False
    )
```
